32 devices in a mesh: fs: 8 (over z, y), tp: 4 (over x, core).
Axes of the slice: x: 2, y: 2, z: 4, core: 2. Of those that a mesh axis runs over, the one named last changes fastest.
Arguments:
- tokens: bfloat16 [8192, 2048], P('fs', 'tp'), may hold values from -6 to 6
- mix_gain: float32 [2048], replicated, may hold values from 0.1 to 1.9
- in_weight: float32 [2048, 1024], P('fs', 'tp'), may hold values from -0.125 to 0.125
- in_scale: float32 [1024], P('tp'), may hold values from 0.4 to 2.5
- out_weight: float32 [1024, 2048], P('tp', 'fs'), may hold values from -0.1875 to 0.1875
- out_scale: float32 [2048], P('fs'), may hold values from 0.4 to 2.5
- ffn_gain: float32 [2048], replicated, may hold values from 0.1 to 1.9
- gate_weight: float32 [2048, 6144], P('fs', 'tp'), may hold values from -0.125 to 0.125
- gate_scale: float32 [6144], P('tp'), may hold values from 0.4 to 2.5
- up_weight: float32 [2048, 6144], P('fs', 'tp'), may hold values from -0.125 to 0.125
- up_scale: float32 [6144], P('tp'), may hold values from 0.4 to 2.5
- down_weight: float32 [6144, 2048], P('tp', 'fs'), may hold values from -0.078125 to 0.078125
- down_scale: float32 [2048], P('fs'), may hold values from 0.4 to 2.5
Outputs:
- layer_out: bfloat16 [8192, 2048], P('fs', 'tp')
The draws below stay inside these ranges and needn't reach their ends.
All inputs are finite; a program needn't handle non-finite values.
Results may differ from the reference program's by a relative error of at most 0.023.
Values may be sent and summed in bfloat16 or wider, within the bound.
A program may use at most 128 MiB of HBM per device.

```python
import math
import jax
import jax.numpy as jnp
from jax import lax

D = 2048
PW = 1024
FF = 6144
GROUPS = 4
GRID_W = 64
ROWS = 16
TOKENS = 8192
GC = 256
PW_DEV = 256
FF_DEV = 1536


def levels(key, shape, cuts, smallest, top_value):
    loudness = 1.0
    for axis_at, blocks in cuts:
        steps = jax.random.uniform(jax.random.fold_in(jax.random.fold_in(key, 6), axis_at), (blocks,), jnp.float32, smallest / len(cuts), top_value / len(cuts))
        loudness = loudness * jnp.repeat(jnp.exp(steps), shape[axis_at] // blocks).reshape((-1,) + (1,) * (len(shape) - 1 - axis_at))
    return loudness


def centred(stream_key, dims, width, most, split=(), kind=jnp.bfloat16):
    level = levels(stream_key, dims, split, -0.22, 0.18) if split else 1.0
    result = jax.random.normal(stream_key, dims, jnp.float32) * width * level
    return jnp.minimum(jnp.maximum(result, -most), most).astype(kind)


def setup_inputs(seed: int = 0) -> dict:
    splits = jax.random.split(jax.random.key(seed), 14)
    return {
        "tokens": centred(splits[0], (TOKENS, D), 1.0, 6.0, ((0, 8), (1, 4))),
        "mix_gain": jnp.clip(1.0 + 0.18 * jax.random.normal(splits[1], (D,), jnp.float32), 0.1, 1.9),
        "in_weight": centred(splits[2], (D, PW), D ** -0.5, 0.125, ((0, 8), (1, 4)), jnp.float32),
        "in_scale": jnp.clip(jnp.exp(math.log(2.5) - 1.8325814 * jax.random.uniform(splits[3], (PW,), jnp.float32) ** levels(splits[3], (PW,), ((0, 4),), -0.2, 0.2)), 0.4, 2.5),
        "out_weight": centred(splits[4], (PW, D), PW ** -0.5, 0.1875, ((0, 4), (1, 8)), jnp.float32),
        "out_scale": jnp.clip(jnp.exp(math.log(2.5) - 1.8325814 * jax.random.uniform(splits[5], (D,), jnp.float32) ** levels(splits[5], (D,), ((0, 8),), -0.2, 0.2)), 0.4, 2.5),
        "ffn_gain": jnp.clip(1.0 + 0.18 * jax.random.normal(splits[6], (D,), jnp.float32), 0.1, 1.9),
        "gate_weight": centred(splits[7], (D, FF), D ** -0.5, 0.125, ((0, 8), (1, 4)), jnp.float32),
        "gate_scale": jnp.clip(jnp.exp(math.log(2.5) - 1.8325814 * jax.random.uniform(splits[8], (FF,), jnp.float32) ** levels(splits[8], (FF,), ((0, 4),), -0.2, 0.2)), 0.4, 2.5),
        "up_weight": centred(splits[9], (D, FF), D ** -0.5, 0.125, ((0, 8), (1, 4)), jnp.float32),
        "up_scale": jnp.clip(jnp.exp(math.log(2.5) - 1.8325814 * jax.random.uniform(splits[10], (FF,), jnp.float32) ** levels(splits[10], (FF,), ((0, 4),), -0.2, 0.2)), 0.4, 2.5),
        "down_weight": centred(splits[11], (FF, D), FF ** -0.5, 0.078125, ((0, 4), (1, 8)), jnp.float32),
        "down_scale": jnp.clip(jnp.exp(math.log(2.5) - 1.8325814 * jax.random.uniform(splits[12], (D,), jnp.float32) ** levels(splits[12], (D,), ((0, 8),), -0.2, 0.2)), 0.4, 2.5),
    }


WINDOWS = (2, 4, 8, 16)
EPSILON = 1e-06

def box_mean(values, window, along):
    length = values.shape[along]
    position = jnp.arange(length, dtype=jnp.int32)
    lower_end = jnp.clip(position - window // 2, 0, length).astype(jnp.int32)
    upper_end = jnp.clip(position + (window - window // 2), 0, length).astype(jnp.int32)
    padding = [(0, 0)] * values.ndim
    padding[along] = (1, 0)
    running = jnp.pad(jnp.cumsum(values, axis=along), padding)
    summed = jnp.take(running, upper_end, axis=along) - jnp.take(running, lower_end, axis=along)
    shaped = [1] * values.ndim
    shaped[along] = length
    return summed / (upper_end - lower_end).astype(jnp.float32).reshape(shaped)

def norm_input(stream, gain):
    inverse_rms = lax.rsqrt(lax.optimization_barrier(jnp.mean(stream * stream, axis=-1, keepdims=True)) + EPSILON)
    return ((stream * gain).astype(jnp.bfloat16), inverse_rms)

def block_sum(hidden, weight, scale, extent):
    total = jnp.zeros((hidden.shape[0], weight.shape[1]), jnp.float32)
    for member in range(hidden.shape[1] // extent):
        term = jnp.dot(hidden[:, member * extent:(member + 1) * extent], weight[member * extent:(member + 1) * extent], preferred_element_type=jnp.float32) * scale
        total = total + term.astype(jnp.bfloat16).astype(jnp.float32)
    return total

def reference(tokens, mix_gain, in_weight, in_scale, out_weight, out_scale, ffn_gain, gate_weight, gate_scale, up_weight, up_scale, down_weight, down_scale):
    stream = tokens.astype(jnp.float32)
    normed, inverse_rms = norm_input(stream, mix_gain)
    channels = jnp.dot(normed, in_weight.astype(jnp.bfloat16), preferred_element_type=jnp.float32) * inverse_rms * in_scale
    lattice = channels.reshape(-1, ROWS, GRID_W, GROUPS, GC)
    differences = []
    for group in range(GROUPS):
        values = lattice[:, :, :, group]
        smoothed = box_mean(box_mean(values, WINDOWS[group], 2), WINDOWS[group], 1)
        differences.append(smoothed - values)
    pooled = jnp.stack(differences, axis=3).reshape(TOKENS, PW).astype(jnp.bfloat16)
    mixed = block_sum(pooled, out_weight.astype(jnp.bfloat16), out_scale, PW_DEV)
    residual = (stream + mixed).astype(jnp.bfloat16)
    normed_ffn, inverse_ffn = norm_input(residual.astype(jnp.float32), ffn_gain)
    gate_value = jnp.dot(normed_ffn, gate_weight.astype(jnp.bfloat16), preferred_element_type=jnp.float32) * inverse_ffn * gate_scale
    up_value = jnp.dot(normed_ffn, up_weight.astype(jnp.bfloat16), preferred_element_type=jnp.float32) * inverse_ffn * up_scale
    hidden = (jax.nn.silu(gate_value) * up_value).astype(jnp.bfloat16)
    channel_out = block_sum(hidden, down_weight.astype(jnp.bfloat16), down_scale, FF_DEV)
    return (residual.astype(jnp.float32) + channel_out).astype(jnp.bfloat16)
```

```python
import jax
import jax.numpy as jnp
from jax import lax
from jax.experimental import pallas as pl
from jax.experimental.pallas import tpu as pltpu
from jax.sharding import PartitionSpec as P

GROUPS = 4
GRID_W = 64
GC = 256
WINDOWS = (2, 4, 8, 16)
EPSILON = 1e-06


IN_SPECS = (
    P("fs", "tp"),
    P(),
    P("fs", "tp"),
    P("tp"),
    P("tp", "fs"),
    P("fs"),
    P(),
    P("fs", "tp"),
    P("tp"),
    P("fs", "tp"),
    P("tp"),
    P("tp", "fs"),
    P("fs"),
)


def box_matrix(length, window):
    position = jnp.arange(length, dtype=jnp.int32)
    lower_end = jnp.clip(position - window // 2, 0, length)
    upper_end = jnp.clip(position + (window - window // 2), 0, length)
    inside = (position[None, :] >= lower_end[:, None]) & (position[None, :] < upper_end[:, None])
    return inside.astype(jnp.float32) / (upper_end - lower_end).astype(jnp.float32)[:, None]


def smooth(lattice, window):
    across = jnp.einsum(
        "jk,akc->ajc", box_matrix(GRID_W, window), lattice, precision=lax.Precision.HIGHEST
    )
    return jnp.einsum(
        "ab,bjc->ajc",
        box_matrix(lattice.shape[0], window),
        across,
        precision=lax.Precision.HIGHEST,
    )


def pooled_differences(channels, channel_offset):
    tokens_here, extent = channels.shape
    lattice = channels.reshape(tokens_here // GRID_W, GRID_W, extent)
    if GC % extent == 0:
        result = smooth(lattice, jnp.asarray(WINDOWS, jnp.int32)[channel_offset // GC])
    else:
        group_of = (channel_offset + jnp.arange(extent, dtype=jnp.int32)) // GC
        result = jnp.zeros_like(lattice)
        for group in range(GROUPS):
            result = jnp.where(
                (group_of == group)[None, None, :], smooth(lattice, WINDOWS[group]), result
            )
    return (result - lattice).reshape(tokens_here, extent).astype(jnp.bfloat16)


class Grid:
    def __init__(self, fs, tp):
        self.ys = max(tp // 2, 1)
        self.zs = fs // self.ys
        index = lax.axis_index("fs")
        self.z, self.y = index // self.ys, index % self.ys

    def gather(self, block):
        rows = []
        for s in range(self.zs):
            pairs = [
                (z * self.ys + y, (z + s) % self.zs * self.ys + y)
                for z in range(self.zs)
                for y in range(self.ys)
            ]
            rows.append(lax.ppermute(block, "fs", pairs) if s else block)
        found = []
        for s, row in enumerate(rows):
            for t in range(self.ys):
                pairs = [
                    (z * self.ys + y, z * self.ys + (y + t) % self.ys)
                    for z in range(self.zs)
                    for y in range(self.ys)
                ]
                item = lax.ppermute(row, "fs", pairs) if t else row
                index = lax.rem(self.z - s + self.zs, self.zs) * self.ys + lax.rem(
                    self.y - t + self.ys, self.ys
                )
                found.append((index, item))
        return found


def stack(pieces):
    shape = (len(pieces),) + pieces[0][1].shape
    result = jnp.zeros(shape, pieces[0][1].dtype)
    for index, item in pieces:
        result = lax.dynamic_update_index_in_dim(result, item, index, 0)
    return result


def rows_of(pieces):
    whole = stack(pieces)
    return whole.reshape(whole.shape[0] * whole.shape[1], whole.shape[2])


def fold_rows(features, gain, weights):
    widened = lax.all_gather(features, "tp", axis=1, tiled=True)
    widened = widened.astype(jnp.float32)
    inverse_rms = lax.rsqrt(jnp.mean(widened * widened, axis=1) + EPSILON)[:, None]
    scaled = (widened * gain).astype(jnp.bfloat16)
    return tuple(
        jnp.dot(scaled, weight, preferred_element_type=jnp.float32) * inverse_rms
        for weight in weights
    )


def column_product(hidden, pieces):
    terms = stack(
        [
            (index, jnp.dot(hidden, item, preferred_element_type=jnp.float32).astype(jnp.bfloat16))
            for index, item in pieces
        ]
    )
    mine = lax.psum_scatter(terms, "tp", scatter_dimension=0, tiled=True)
    return mine.transpose(1, 0, 2).reshape(hidden.shape[0], -1).astype(jnp.float32)


def low(weight, scale=None):
    weight = weight.astype(jnp.bfloat16)
    if scale is None:
        return weight
    return (weight.astype(jnp.float32) * scale).astype(jnp.bfloat16)


def general(mesh):
    fs, tp = mesh.shape["fs"], mesh.shape["tp"]

    def layer(
        tokens,
        mix_gain,
        in_weight,
        in_scale,
        out_weight,
        out_scale,
        ffn_gain,
        gate_weight,
        gate_scale,
        up_weight,
        up_scale,
        down_weight,
        down_scale,
    ):
        grid = Grid(fs, tp)
        wide = gate_weight.shape[1]
        both_pieces = grid.gather(jnp.concatenate([low(gate_weight), low(up_weight)], axis=1))
        down_pieces = grid.gather(low(down_weight, down_scale))
        small = lax.all_gather(
            jnp.stack([low(in_weight), low(out_weight, out_scale)]), "fs", axis=0
        )
        in_full = small[:, 0].reshape(-1, in_weight.shape[1])
        out_pieces = [(j, small[j, 1]) for j in range(fs)]
        (channels,) = fold_rows(tokens, mix_gain, (in_full,))
        channels = channels * in_scale
        pooled = pooled_differences(channels, lax.axis_index("tp") * channels.shape[1])
        mixed = column_product(pooled, out_pieces)
        residual = (tokens.astype(jnp.float32) + mixed).astype(jnp.bfloat16)
        (both,) = fold_rows(residual, ffn_gain, (rows_of(both_pieces),))
        gate_value = both[:, :wide] * gate_scale
        up_value = both[:, wide:] * up_scale
        hidden = (jax.nn.silu(gate_value) * up_value).astype(jnp.bfloat16)
        channel_out = column_product(hidden, down_pieces)
        return (residual.astype(jnp.float32) + channel_out).astype(jnp.bfloat16)

    return jax.shard_map(
        layer, mesh=mesh, in_specs=IN_SPECS, out_specs=P("fs", "tp"), check_vma=False
    )


class Place:
    def __init__(self):
        index, column = lax.axis_index("fs"), lax.axis_index("tp")
        z, self.y = index // 2, index % 2
        self.zh, self.zl = z // 2, z % 2
        self.x, self.c = column // 2, column % 2
        self.index, self.column = index, column
        self.to_x = {"tp": (1 - self.x) * 2 + self.c}
        self.to_c = {"tp": self.x * 2 + 1 - self.c}
        self.to_y = {"fs": z * 2 + 1 - self.y}
        self.to_zl = {"fs": (self.zh * 2 + 1 - self.zl) * 2 + self.y}
        self.to_zh = {"fs": ((1 - self.zh) * 2 + self.zl) * 2 + self.y}

    def slot(self, dh, dl, dy):
        zh, zl, y = (self.zh + dh) % 2, (self.zl + dl) % 2, (self.y + dy) % 2
        return (zh * 2 + zl) * 2 + y


class Mail:
    def __init__(self):
        self.started = []

    def send(self, source, target, send_sem, recv_sem, device):
        copy = pltpu.make_async_remote_copy(
            src_ref=source,
            dst_ref=target,
            send_sem=send_sem,
            recv_sem=recv_sem,
            device_id=device,
            device_id_type=pl.DeviceIdType.MESH,
        )
        copy.start()
        self.started.append(copy)

    def arrived(self, target, recv_sem):
        pltpu.make_async_copy(target, target, recv_sem).wait()

    def close(self):
        for copy in self.started:
            copy.wait_send()
        self.started = []


class Gather:
    def __init__(self, mail, place, kind, target, sends, recvs):
        self.mail, self.place, self.kind = mail, place, kind
        self.target, self.sends, self.recvs = target, sends, recvs
        self.count = 0

    def pass_on(self, source, slot, device):
        self.mail.send(
            source,
            self.target(slot),
            self.sends.at[self.kind, self.count],
            self.recvs.at[self.kind, slot],
            device,
        )
        self.count += 1

    def forward(self, slot, *devices):
        self.mail.arrived(self.target(slot), self.recvs.at[self.kind, slot])
        for device in devices:
            self.pass_on(self.target(slot), slot, device)

    def keep(self, own, sem):
        copy = pltpu.make_async_copy(own, self.target(self.place.index), sem)
        copy.start()
        return copy

    def rows_y(self):
        for dh, dl in ((0, 0), (0, 1), (1, 0), (1, 1)):
            self.forward(self.place.slot(dh, dl, 1))


class WholeGather(Gather):
    def start(self, own):
        p = self.place
        self.pass_on(own, p.index, p.to_zh)
        self.pass_on(own, p.index, p.to_zl)
        self.pass_on(own, p.index, p.to_y)

    def on_zh(self):
        p = self.place
        self.forward(p.slot(1, 0, 0), p.to_zl, p.to_y)

    def on_zl(self):
        p = self.place
        self.forward(p.slot(0, 1, 0), p.to_y)
        self.forward(p.slot(1, 1, 0), p.to_y)


class HalfGather(Gather):
    def start(self, own, other):
        p = self.place
        self.pass_on(other, p.index, p.to_zl)
        self.pass_on(own, p.index, p.to_zh)
        self.pass_on(own, p.index, p.to_y)

    def on_zl(self):
        p = self.place
        self.forward(p.slot(0, 1, 0), p.to_zh, p.to_y)

    def on_zh(self, dl):
        p = self.place
        self.forward(p.slot(1, dl, 0), p.to_y)


def lanes(start, size):
    return pl.ds(pl.multiple_of(start, 128), size)


def fused(
    tok, w_in, w_out, w_gu, w_dn, out,
    tokens, res, in_all, out_all, gu_all, dn_all, hid, mask, chan, high, low_part, pooled,
    mix_cs, mix_cr, mix_own, mix_xs, mix_xr,
    sum_cs, sum_cr, sum_xs, sum_xr, sum_zs, sum_zr, inv, done,
    local_sem, w_send, w_recv, t_send, t_recv, r_send, r_recv, m_send, m_recv, s_send, s_recv,
):
    rows, features = tokens.shape
    cols = tok.shape[1]
    block = w_in.shape[0]
    half = gu_all.shape[2] // 2
    chunk = rows // 4
    tall = rows // 2
    p, mail = Place(), Mail()

    def kept(kind):
        return {
            0: lambda j: in_all.at[pl.ds(pl.multiple_of(j * block, 16), block), :],
            1: lambda j: out_all.at[j],
            2: lambda j: gu_all.at[0, pl.ds(pl.multiple_of(j * block, 16), block), :],
            3: lambda j: gu_all.at[1, pl.ds(pl.multiple_of(j * block, 16), block), :],
            4: lambda j: dn_all.at[j],
        }[kind]

    g_in, g_out = (WholeGather(mail, p, k, kept(k), w_send, w_recv) for k in (0, 1))
    g_gu = [HalfGather(mail, p, 2 + q, kept(2 + q), w_send, w_recv) for q in (0, 1)]
    g_dn = HalfGather(mail, p, 4, kept(4), w_send, w_recv)

    def piece(k):
        return pl.ds(k * chunk, chunk)

    def column_of(dx, dc):
        return ((p.x + dx) % 2) * 2 + (p.c + dc) % 2

    g_in.start(w_in)
    for k in range(4):
        own = tok.at[piece(k), :]
        at = tokens.at[piece(k), lanes(p.column * cols, cols)]
        mail.send(own, at, t_send.at[0, k], t_recv.at[p.column, k], p.to_x)
        mail.send(own, at, t_send.at[1, k], t_recv.at[p.column, k], p.to_c)
    g_out.start(w_out)
    copies = [
        pltpu.make_async_copy(tok, tokens.at[:, lanes(p.column * cols, cols)], local_sem.at[0])
    ]
    copies[0].start()
    copies.append(g_in.keep(w_in, local_sem.at[1]))
    copies.append(g_out.keep(w_out, local_sem.at[2]))
    for q in (0, 1):
        copies.append(g_gu[q].keep(w_gu.at[p.zl, q], local_sem.at[3 + q]))
    copies.append(g_dn.keep(w_dn.at[p.zl], local_sem.at[5]))

    window = lax.shift_left(2, p.column * block // GC)
    below = window // 2
    above = window - below

    def mask_rows(i, _):
        cell = i * chunk // 2 + lax.broadcasted_iota(jnp.int32, (chunk // 2, rows), 0)
        other = lax.broadcasted_iota(jnp.int32, (chunk // 2, rows), 1)
        dr = other // GRID_W - cell // GRID_W
        dc = other % GRID_W - cell % GRID_W
        inside = (dr >= -below) & (dr < above) & (dc >= -below) & (dc < above)
        at = pl.ds(pl.multiple_of(i * (chunk // 2), 16), chunk // 2)
        mask[at, :] = jnp.where(inside, 1.0, 0.0).astype(jnp.bfloat16)
        return 0

    lax.fori_loop(0, 8, mask_rows, 0)

    g_in.on_zh()
    g_out.on_zh()
    g_in.on_zl()
    g_out.on_zl()
    for q in (0, 1):
        g_gu[q].start(w_gu.at[p.zl, q], w_gu.at[1 - p.zl, q])

    def token_at(column, k):
        return tokens.at[piece(k), lanes(column * cols, cols)]

    for k in range(4):
        column = column_of(1, 0)
        mail.arrived(token_at(column, k), t_recv.at[column, k])
        mail.send(
            token_at(column, k), token_at(column, k), t_send.at[2, k], t_recv.at[column, k], p.to_c
        )
    for copy in copies:
        copy.wait()
    for dx in (0, 1):
        for k in range(4):
            column = column_of(dx, 1)
            mail.arrived(token_at(column, k), t_recv.at[column, k])
    g_in.rows_y()

    def channel_rows(i, _):
        at = pl.ds(pl.multiple_of(i * chunk, 16), chunk)
        wide = tokens[at, :]
        square = wide.astype(jnp.float32)
        scale = lax.rsqrt(jnp.sum(square * square, axis=1, keepdims=True) / features + EPSILON)
        value = jnp.dot(wide, in_all[...], preferred_element_type=jnp.float32) * scale
        chan[at, :] = value
        first = value.astype(jnp.bfloat16)
        high[at, :] = first
        low_part[at, :] = (value - first.astype(jnp.float32)).astype(jnp.bfloat16)
        return 0

    lax.fori_loop(0, 4, channel_rows, 0)

    def extent(position, length):
        upper = jnp.minimum(position + above, length)
        return upper - jnp.maximum(position - below, 0)

    def pool_rows(i, _):
        at = pl.ds(pl.multiple_of(i * chunk, 16), chunk)
        inside = mask[at, :]
        total = jnp.dot(inside, high[...], preferred_element_type=jnp.float32) + jnp.dot(
            inside, low_part[...], preferred_element_type=jnp.float32
        )
        cell = i * chunk + lax.broadcasted_iota(jnp.int32, (chunk, block), 0)
        cells = extent(cell // GRID_W, rows // GRID_W) * extent(cell % GRID_W, GRID_W)
        pooled[at, :] = (total / cells.astype(jnp.float32) - chan[at, :]).astype(jnp.bfloat16)
        return 0

    lax.fori_loop(0, 4, pool_rows, 0)

    g_gu[0].on_zl()
    g_out.rows_y()

    for k in range(4):
        part = pooled[piece(k), :]
        for dx in (0, 1):
            for dc in (0, 1):
                target = mix_own if dc == 0 else mix_cs
                for side in (0, 1):
                    j = column_of(dx, dc) * 2 + side
                    term = jnp.dot(part, out_all[j], preferred_element_type=jnp.float32)
                    target[k, dx, :, side * block:(side + 1) * block] = term.astype(jnp.bfloat16)
        mail.send(mix_cs.at[k], mix_cr.at[k], m_send.at[0, k], m_recv.at[0, k], p.to_c)

    def both(k, dx):
        return mix_own[k, dx].astype(jnp.float32) + mix_cr[k, dx].astype(jnp.float32)

    for k in range(4):
        mail.arrived(mix_cr.at[k], m_recv.at[0, k])
        mix_xs[k] = both(k, 1).astype(jnp.bfloat16)
        mail.send(mix_xs.at[k], mix_xr.at[k], m_send.at[1, k], m_recv.at[1, k], p.to_x)
    g_gu[1].on_zl()
    g_dn.start(w_dn.at[p.zl], w_dn.at[1 - p.zl])

    def res_at(dz, column, k):
        return res.at[(p.zl + dz) % 2, piece(k), lanes(column * cols, cols)]

    def res_send(dz, column, k, lane, device):
        here = res_at(dz, column, k)
        sem = ((p.zl + dz) % 2) * 4 + column
        mail.send(here, here, r_send.at[lane, k], r_recv.at[sem, k], device)

    def res_wait(dz, column, k):
        sem = ((p.zl + dz) % 2) * 4 + column
        mail.arrived(res_at(dz, column, k), r_recv.at[sem, k])

    for k in range(4):
        mail.arrived(mix_xr.at[k], m_recv.at[1, k])
        mine = lanes(p.column * cols, cols)
        total = both(k, 0) + mix_xr[k].astype(jnp.float32)
        total = total + tokens[piece(k), mine].astype(jnp.float32)
        res[p.zl, piece(k), mine] = total.astype(jnp.bfloat16)
        res_send(0, p.column, k, 0, p.to_x)
        res_send(0, p.column, k, 1, p.to_zl)
        res_send(0, p.column, k, 2, p.to_c)
        if k == 1:
            g_gu[0].on_zh(0)

    for k in range(4):
        res_wait(1, p.column, k)
        if k < 2:
            res_send(1, p.column, k, 3, p.to_x)
        res_send(1, p.column, k, 4, p.to_c)
    g_gu[1].on_zh(0)
    across = column_of(1, 0)
    for k in range(4):
        res_wait(0, across, k)
        if k >= 2:
            res_send(0, across, k, 3, p.to_zl)
        res_send(0, across, k, 5, p.to_c)
    g_gu[0].on_zh(1)
    g_dn.on_zl()
    for k in range(4):
        res_wait(1, across, k)
        res_send(1, across, k, 6, p.to_c)
    g_gu[1].on_zh(1)
    for dz in (0, 1):
        for dx in (0, 1):
            for k in range(4):
                res_wait(dz, column_of(dx, 1), k)

    def norm_rows(i, _):
        at = pl.ds(pl.multiple_of((i % 4) * chunk, 16), chunk)
        square = res[i // 4, at, :].astype(jnp.float32)
        scale = lax.rsqrt(jnp.sum(square * square, axis=1, keepdims=True) / features + EPSILON)
        inv[i // 4, at, :] = jnp.broadcast_to(scale, (chunk, inv.shape[2]))
        return 0

    lax.fori_loop(0, 8, norm_rows, 0)
    for q in (0, 1):
        g_gu[q].rows_y()

        def hidden_rows(i, _):
            at = pl.ds(pl.multiple_of((i % 4) * chunk, 16), chunk)
            scale = inv[i // 4, at, :1]
            value = jnp.dot(
                res[i // 4, at, :], gu_all[q], preferred_element_type=jnp.float32
            ) * scale
            gate, up = value[:, :half], value[:, half:]
            unit = gate / (1.0 + jnp.exp(-gate)) * up
            hid[i // 4, at, q * half:(q + 1) * half] = unit.astype(jnp.bfloat16)
            return 0

        lax.fori_loop(0, 8, hidden_rows, 0)
        if q == 0:
            g_dn.on_zh(0)
    g_dn.on_zh(1)

    def sum_own(u, dx):
        return tokens.at[pl.ds((u % 2) * tall, tall), pl.ds((u // 2 * 2 + dx) * block, block)]

    def stage_core(u):
        dy, dz, k = u // 4, 1 - u // 2 % 2, u % 2
        part = hid[(p.zl + dz) % 2, pl.ds(k * tall, tall), :]
        for dx in (0, 1):
            for dc in (0, 1):
                j = column_of(dx, dc) * 2 + (p.y + dy) % 2
                term = jnp.dot(part, dn_all[j], preferred_element_type=jnp.float32)
                if dc == 0:
                    sum_own(u, dx)[...] = term.astype(jnp.bfloat16)
                else:
                    sum_cs[u, dx] = term.astype(jnp.bfloat16)
        mail.send(sum_cs.at[u], sum_cr.at[u], s_send.at[0, u], s_recv.at[0, u], p.to_c)

    def pair(u, dx):
        return sum_own(u, dx)[...].astype(jnp.float32) + sum_cr[u, dx].astype(jnp.float32)

    def stage_x(u):
        mail.arrived(sum_cr.at[u], s_recv.at[0, u])
        sum_xs[u] = pair(u, 1).astype(jnp.bfloat16)
        mail.send(sum_xs.at[u], sum_xr.at[u], s_send.at[1, u], s_recv.at[1, u], p.to_x)

    mail.close()
    for u in range(8):
        if u == 4:
            g_dn.rows_y()
        stage_core(u)
        if u:
            stage_x(u - 1)
    stage_x(7)

    for u in range(8):
        dy, dz, k = u // 4, 1 - u // 2 % 2, u % 2
        mail.arrived(sum_xr.at[u], s_recv.at[1, u])
        total = pair(u, 0) + sum_xr[u].astype(jnp.float32)
        n = dy * 2 + k
        if dz:
            sum_zs[n] = total.astype(jnp.bfloat16)
            mail.send(sum_zs.at[n], sum_zr.at[n], s_send.at[2, n], s_recv.at[2, n], p.to_zl)
        else:
            mail.arrived(sum_zr.at[n], s_recv.at[2, n])
            side = (p.y + dy) % 2 * block
            at = pl.ds(k * tall, tall)
            total = total + sum_zr[n].astype(jnp.float32)
            total = total + res[p.zl, at, lanes(p.column * cols + side, block)].astype(jnp.float32)
            done[at, lanes(side, block)] = total.astype(jnp.bfloat16)
    copy = pltpu.make_async_copy(done, out, local_sem.at[0])
    copy.start()
    mail.close()
    copy.wait()


def paired(mesh):
    fs, tp = mesh.shape["fs"], mesh.shape["tp"]

    def local(
        tokens,
        mix_gain,
        in_weight,
        in_scale,
        out_weight,
        out_scale,
        ffn_gain,
        gate_weight,
        gate_scale,
        up_weight,
        up_scale,
        down_weight,
        down_scale,
    ):
        rows, cols = tokens.shape
        depth, block = in_weight.shape
        wide = gate_weight.shape[1]
        start = lax.axis_index("fs") * depth
        mix_rows = lax.dynamic_slice(mix_gain, (start,), (depth,))[:, None]
        ffn_rows = lax.dynamic_slice(ffn_gain, (start,), (depth,))[:, None]
        w_in = low(in_weight, mix_rows * in_scale)
        w_out = low(out_weight, out_scale)
        quarters = [
            low(weight, ffn_rows * scale).reshape(depth, 2, 2, wide // 4)
            for weight, scale in ((gate_weight, gate_scale), (up_weight, up_scale))
        ]
        w_gu = jnp.concatenate(quarters, axis=3).transpose(1, 2, 0, 3)
        w_dn = low(down_weight, down_scale).reshape(2, wide // 2, block)
        features = cols * tp
        low_type = jnp.bfloat16
        tall = rows // 2
        buffers = [
            ((rows, features), low_type),
            ((2, rows, features), low_type),
            ((features, block), low_type),
            ((fs, block, block), low_type),
            ((2, features, wide // 2), low_type),
            ((fs, wide // 2, block), low_type),
            ((2, rows, wide // 2), low_type),
            ((rows, rows), low_type),
            ((rows, block), jnp.float32),
            ((rows, block), low_type),
            ((rows, block), low_type),
            ((rows, block), low_type),
            ((4, 2, rows // 4, cols), low_type),
            ((4, 2, rows // 4, cols), low_type),
            ((4, 2, rows // 4, cols), low_type),
            ((4, rows // 4, cols), low_type),
            ((4, rows // 4, cols), low_type),
            ((8, 2, tall, block), low_type),
            ((8, 2, tall, block), low_type),
            ((8, tall, block), low_type),
            ((8, tall, block), low_type),
            ((4, tall, block), low_type),
            ((4, tall, block), low_type),
            ((2, rows, 128), jnp.float32),
            ((rows, cols), low_type),
        ]
        semaphores = [(6,), (5, 7), (5, fs), (3, 4), (tp, 4), (7, 4), (2 * tp, 4), (2, 4), (2, 4)]
        semaphores += [(3, 8), (3, 8)]
        anywhere = pl.BlockSpec(memory_space=pl.ANY)
        return pl.pallas_call(
            fused,
            out_shape=jax.ShapeDtypeStruct((rows, cols), low_type),
            in_specs=[anywhere] * 5,
            out_specs=anywhere,
            scratch_shapes=[pltpu.VMEM(shape, kind) for shape, kind in buffers]
            + [pltpu.SemaphoreType.DMA(shape) for shape in semaphores],
            compiler_params=pltpu.CompilerParams(
                has_side_effects=True, vmem_limit_bytes=67043328
            ),
        )(tokens, w_in, w_out, w_gu, w_dn)

    return jax.shard_map(
        local, mesh=mesh, in_specs=IN_SPECS, out_specs=P("fs", "tp"), check_vma=False
    )


def solution(mesh):
    fs, tp = mesh.shape["fs"], mesh.shape["tp"]
    xs = max(tp // 2, 1)
    return paired(mesh) if (xs, fs // xs) == (2, 4) else general(mesh)
```

```python
import jax
import jax.numpy as jnp
from jax import lax
from jax.experimental import pallas as pl
from jax.experimental.pallas import tpu as pltpu
from jax.sharding import PartitionSpec as P

GROUPS = 4
GRID_W = 64
GC = 256
WINDOWS = (2, 4, 8, 16)
EPSILON = 1e-06


IN_SPECS = (
    P("fs", "tp"),
    P(),
    P("fs", "tp"),
    P("tp"),
    P("tp", "fs"),
    P("fs"),
    P(),
    P("fs", "tp"),
    P("tp"),
    P("fs", "tp"),
    P("tp"),
    P("tp", "fs"),
    P("fs"),
)


def box_matrix(length, window):
    position = jnp.arange(length, dtype=jnp.int32)
    lower_end = jnp.clip(position - window // 2, 0, length)
    upper_end = jnp.clip(position + (window - window // 2), 0, length)
    inside = (position[None, :] >= lower_end[:, None]) & (position[None, :] < upper_end[:, None])
    return inside.astype(jnp.float32) / (upper_end - lower_end).astype(jnp.float32)[:, None]


def smooth(lattice, window):
    across = jnp.einsum(
        "jk,akc->ajc", box_matrix(GRID_W, window), lattice, precision=lax.Precision.HIGHEST
    )
    return jnp.einsum(
        "ab,bjc->ajc",
        box_matrix(lattice.shape[0], window),
        across,
        precision=lax.Precision.HIGHEST,
    )


def pooled_differences(channels, channel_offset):
    tokens_here, extent = channels.shape
    lattice = channels.reshape(tokens_here // GRID_W, GRID_W, extent)
    if GC % extent == 0:
        result = smooth(lattice, jnp.asarray(WINDOWS, jnp.int32)[channel_offset // GC])
    else:
        group_of = (channel_offset + jnp.arange(extent, dtype=jnp.int32)) // GC
        result = jnp.zeros_like(lattice)
        for group in range(GROUPS):
            result = jnp.where(
                (group_of == group)[None, None, :], smooth(lattice, WINDOWS[group]), result
            )
    return (result - lattice).reshape(tokens_here, extent).astype(jnp.bfloat16)


class Grid:
    def __init__(self, fs, tp):
        self.ys = max(tp // 2, 1)
        self.zs = fs // self.ys
        index = lax.axis_index("fs")
        self.z, self.y = index // self.ys, index % self.ys

    def gather(self, block):
        rows = []
        for s in range(self.zs):
            pairs = [
                (z * self.ys + y, (z + s) % self.zs * self.ys + y)
                for z in range(self.zs)
                for y in range(self.ys)
            ]
            rows.append(lax.ppermute(block, "fs", pairs) if s else block)
        found = []
        for s, row in enumerate(rows):
            for t in range(self.ys):
                pairs = [
                    (z * self.ys + y, z * self.ys + (y + t) % self.ys)
                    for z in range(self.zs)
                    for y in range(self.ys)
                ]
                item = lax.ppermute(row, "fs", pairs) if t else row
                index = lax.rem(self.z - s + self.zs, self.zs) * self.ys + lax.rem(
                    self.y - t + self.ys, self.ys
                )
                found.append((index, item))
        return found


def stack(pieces):
    shape = (len(pieces),) + pieces[0][1].shape
    result = jnp.zeros(shape, pieces[0][1].dtype)
    for index, item in pieces:
        result = lax.dynamic_update_index_in_dim(result, item, index, 0)
    return result


def rows_of(pieces):
    whole = stack(pieces)
    return whole.reshape(whole.shape[0] * whole.shape[1], whole.shape[2])


def fold_rows(features, gain, weights):
    widened = lax.all_gather(features, "tp", axis=1, tiled=True)
    widened = widened.astype(jnp.float32)
    inverse_rms = lax.rsqrt(jnp.mean(widened * widened, axis=1) + EPSILON)[:, None]
    scaled = (widened * gain).astype(jnp.bfloat16)
    return tuple(
        jnp.dot(scaled, weight, preferred_element_type=jnp.float32) * inverse_rms
        for weight in weights
    )


def column_product(hidden, pieces):
    terms = stack(
        [
            (index, jnp.dot(hidden, item, preferred_element_type=jnp.float32).astype(jnp.bfloat16))
            for index, item in pieces
        ]
    )
    mine = lax.psum_scatter(terms, "tp", scatter_dimension=0, tiled=True)
    return mine.transpose(1, 0, 2).reshape(hidden.shape[0], -1).astype(jnp.float32)


def low(weight, scale=None):
    weight = weight.astype(jnp.bfloat16)
    if scale is None:
        return weight
    return (weight.astype(jnp.float32) * scale).astype(jnp.bfloat16)


def general(mesh):
    fs, tp = mesh.shape["fs"], mesh.shape["tp"]

    def layer(
        tokens,
        mix_gain,
        in_weight,
        in_scale,
        out_weight,
        out_scale,
        ffn_gain,
        gate_weight,
        gate_scale,
        up_weight,
        up_scale,
        down_weight,
        down_scale,
    ):
        grid = Grid(fs, tp)
        wide = gate_weight.shape[1]
        both_pieces = grid.gather(jnp.concatenate([low(gate_weight), low(up_weight)], axis=1))
        down_pieces = grid.gather(low(down_weight, down_scale))
        small = lax.all_gather(
            jnp.stack([low(in_weight), low(out_weight, out_scale)]), "fs", axis=0
        )
        in_full = small[:, 0].reshape(-1, in_weight.shape[1])
        out_pieces = [(j, small[j, 1]) for j in range(fs)]
        (channels,) = fold_rows(tokens, mix_gain, (in_full,))
        channels = channels * in_scale
        pooled = pooled_differences(channels, lax.axis_index("tp") * channels.shape[1])
        mixed = column_product(pooled, out_pieces)
        residual = (tokens.astype(jnp.float32) + mixed).astype(jnp.bfloat16)
        (both,) = fold_rows(residual, ffn_gain, (rows_of(both_pieces),))
        gate_value = both[:, :wide] * gate_scale
        up_value = both[:, wide:] * up_scale
        hidden = (jax.nn.silu(gate_value) * up_value).astype(jnp.bfloat16)
        channel_out = column_product(hidden, down_pieces)
        return (residual.astype(jnp.float32) + channel_out).astype(jnp.bfloat16)

    return jax.shard_map(
        layer, mesh=mesh, in_specs=IN_SPECS, out_specs=P("fs", "tp"), check_vma=False
    )


class Place:
    def __init__(self):
        index, column = lax.axis_index("fs"), lax.axis_index("tp")
        z, self.y = index // 2, index % 2
        self.zh, self.zl = z // 2, z % 2
        self.x, self.c = column // 2, column % 2
        self.index, self.column = index, column
        self.to_x = {"tp": (1 - self.x) * 2 + self.c}
        self.to_c = {"tp": self.x * 2 + 1 - self.c}
        self.to_y = {"fs": z * 2 + 1 - self.y}
        self.to_zl = {"fs": (self.zh * 2 + 1 - self.zl) * 2 + self.y}
        self.to_zh = {"fs": ((1 - self.zh) * 2 + self.zl) * 2 + self.y}

    def slot(self, dh, dl, dy):
        zh, zl, y = (self.zh + dh) % 2, (self.zl + dl) % 2, (self.y + dy) % 2
        return (zh * 2 + zl) * 2 + y


class Mail:
    def __init__(self):
        self.started = []

    def send(self, source, target, send_sem, recv_sem, device):
        copy = pltpu.make_async_remote_copy(
            src_ref=source,
            dst_ref=target,
            send_sem=send_sem,
            recv_sem=recv_sem,
            device_id=device,
            device_id_type=pl.DeviceIdType.MESH,
        )
        copy.start()
        self.started.append(copy)
        return copy

    def arrived(self, target, recv_sem):
        pltpu.make_async_copy(target, target, recv_sem).wait()

    def settle(self, copies):
        for copy in copies:
            copy.wait_send()
        self.started = [copy for copy in self.started if all(copy is not c for c in copies)]

    def close(self):
        self.settle(self.started)


class Gather:
    def __init__(self, mail, place, kind, target, sends, recvs):
        self.mail, self.place, self.kind = mail, place, kind
        self.target, self.sends, self.recvs = target, sends, recvs
        self.count = 0

    def pass_on(self, source, slot, device):
        self.mail.send(
            source,
            self.target(slot),
            self.sends.at[self.kind, self.count],
            self.recvs.at[self.kind, slot],
            device,
        )
        self.count += 1

    def forward(self, slot, *devices):
        self.mail.arrived(self.target(slot), self.recvs.at[self.kind, slot])
        for device in devices:
            self.pass_on(self.target(slot), slot, device)

    def rows_y(self):
        for dh, dl in ((0, 0), (0, 1), (1, 0), (1, 1)):
            self.forward(self.place.slot(dh, dl, 1))


class WholeGather(Gather):
    def start(self, own):
        p = self.place
        self.pass_on(own, p.index, p.to_zh)
        self.pass_on(own, p.index, p.to_zl)
        self.pass_on(own, p.index, p.to_y)

    def on_zh(self):
        p = self.place
        self.forward(p.slot(1, 0, 0), p.to_zl, p.to_y)

    def on_zl(self):
        p = self.place
        self.forward(p.slot(0, 1, 0), p.to_y)
        self.forward(p.slot(1, 1, 0), p.to_y)


class HalfGather(Gather):
    def start_zl(self, other):
        self.pass_on(other, self.place.index, self.place.to_zl)

    def start_zh(self, own):
        self.pass_on(own, self.place.index, self.place.to_zh)

    def start_y(self, own):
        self.pass_on(own, self.place.index, self.place.to_y)

    def start(self, own):
        self.start_zh(own)
        self.start_y(own)

    def on_zl(self):
        p = self.place
        self.forward(p.slot(0, 1, 0), p.to_zh, p.to_y)

    def on_zh(self, dl):
        p = self.place
        self.forward(p.slot(1, dl, 0), p.to_y)


def lanes(start, size):
    return pl.ds(pl.multiple_of(start, 128), size)


def fused(
    tok, w_in, w_out, w_gate, w_up, w_down,
    gain_mix, gain_ffn, s_in, s_out, s_gate, s_up, s_down, out,
    tokens, res, in_all, out_all, gu_all, dn_all, hid, mask, chan, high, low_part, pooled,
    mix_cs, mix_cr, mix_own, mix_xs, mix_xr,
    sum_cs, sum_cr, sum_xs, sum_xr, sum_zs, sum_zr, done,
    f_in, f_out, f_gate, f_up, f_down, gu_other, dn_other,
    local_sem, w_send, w_recv, t_send, t_recv, r_send, r_recv, m_send, m_recv,
    c_send, c_recv, x_send, x_recv, z_send, z_recv,
):
    rows, features = tokens.shape
    cols = tok.shape[1]
    block = w_in.shape[0]
    unit_hidden = dn_all.shape[1]
    half = gu_all.shape[2] // 2
    chunk = rows // 4
    tall = rows // 2
    p, mail = Place(), Mail()

    def kept(kind):
        return {
            0: lambda j: in_all.at[pl.ds(pl.multiple_of(j * block, 16), block), :],
            1: lambda j: out_all.at[j],
            2: lambda j: gu_all.at[0, pl.ds(pl.multiple_of(j * block, 16), block), :],
            3: lambda j: gu_all.at[1, pl.ds(pl.multiple_of(j * block, 16), block), :],
            4: lambda j: dn_all.at[j],
        }[kind]

    g_in, g_out = (WholeGather(mail, p, k, kept(k), w_send, w_recv) for k in (0, 1))
    g_gu = [HalfGather(mail, p, 2 + q, kept(2 + q), w_send, w_recv) for q in (0, 1)]
    g_dn = HalfGather(mail, p, 4, kept(4), w_send, w_recv)

    def piece(k):
        return pl.ds(k * chunk, chunk)

    def column_of(dx, dc):
        return ((p.x + dx) % 2) * 2 + (p.c + dc) % 2

    copies = [
        pltpu.make_async_copy(source, target, local_sem.at[n])
        for n, (source, target) in enumerate((
            (w_in, f_in),
            (w_out, f_out),
            (tok, tokens.at[:, lanes(p.column * cols, cols)]),
            (w_gate, f_gate),
            (w_up, f_up),
            (w_down, f_down),
        ))
    ]
    for copy in copies:
        copy.start()
    barrier = pltpu.get_barrier_semaphore()
    for device in (p.to_c, p.to_x, p.to_y, p.to_zl, p.to_zh):
        pl.semaphore_signal(
            barrier, inc=1, device_id=device, device_id_type=pl.DeviceIdType.MESH
        )
    pl.semaphore_wait(barrier, 5)
    for k in range(4):
        own = tok.at[piece(k), :]
        at = tokens.at[piece(k), lanes(p.column * cols, cols)]
        mail.send(own, at, t_send.at[0, k], t_recv.at[p.column, k], p.to_x)
        mail.send(own, at, t_send.at[1, k], t_recv.at[p.column, k], p.to_c)

    def rounded(weight, scale):
        weight = weight.astype(jnp.bfloat16).astype(jnp.float32)
        return (weight * scale[None, :]).astype(jnp.bfloat16)

    copies[0].wait()
    kept(0)(p.index)[...] = rounded(f_in[...], s_in[...])
    g_in.start(kept(0)(p.index))
    copies[1].wait()
    kept(1)(p.index)[...] = rounded(f_out[...], s_out[...])
    g_out.start(kept(1)(p.index))
    for copy in copies[3:]:
        copy.wait()
    for q in (0, 1):
        for own in (True, False):
            target = kept(2 + q)(p.index) if own else gu_other.at[q]
            at = lanes(((p.zl if own else 1 - p.zl) * 2 + q) * half, half)
            target[:, :half] = rounded(f_gate[:, at], s_gate[at])
            target[:, half:] = rounded(f_up[:, at], s_up[at])
    for own in (True, False):
        target = kept(4)(p.index) if own else dn_other
        at = (p.zl if own else 1 - p.zl) * unit_hidden
        at = pl.ds(pl.multiple_of(at, 16), unit_hidden)
        target[...] = rounded(f_down[at, :], s_down[...])

    window = lax.shift_left(2, p.column * block // GC)
    below = window // 2
    above = window - below

    def mask_rows(i, _):
        cell = i * chunk // 2 + lax.broadcasted_iota(jnp.int32, (chunk // 2, rows), 0)
        other = lax.broadcasted_iota(jnp.int32, (chunk // 2, rows), 1)
        dr = other // GRID_W - cell // GRID_W
        dc = other % GRID_W - cell % GRID_W
        inside = (dr >= -below) & (dr < above) & (dc >= -below) & (dc < above)
        at = pl.ds(pl.multiple_of(i * (chunk // 2), 16), chunk // 2)
        mask[at, :] = jnp.where(inside, 1.0, 0.0).astype(jnp.bfloat16)
        return 0

    lax.fori_loop(0, 8, mask_rows, 0)

    g_in.on_zh()
    g_out.on_zh()
    g_in.on_zl()
    g_out.on_zl()
    for q in (0, 1):
        g_gu[q].start_zl(gu_other.at[q])
    for q in (0, 1):
        g_gu[q].start(kept(2 + q)(p.index))
    g_dn.start_y(kept(4)(p.index))

    def token_at(column, k):
        return tokens.at[piece(k), lanes(column * cols, cols)]

    passed = []
    for k in range(4):
        column = column_of(1, 0)
        here = token_at(column, k)
        mail.arrived(here, t_recv.at[column, k])
        passed.append(mail.send(here, here, t_send.at[2, k], t_recv.at[column, k], p.to_c))
    copies[2].wait()
    for dx in (0, 1):
        for k in range(4):
            column = column_of(dx, 1)
            mail.arrived(token_at(column, k), t_recv.at[column, k])
    g_in.rows_y()

    def normed(wide, gain):
        square = wide * wide
        scale = lax.rsqrt(jnp.sum(square, axis=1, keepdims=True) / features + EPSILON)
        return (wide * gain[...][None, :]).astype(jnp.bfloat16), scale

    def channel_rows(i, _):
        at = pl.ds(pl.multiple_of(i * chunk, 16), chunk)
        wide, scale = normed(tokens[at, :].astype(jnp.float32), gain_mix)
        value = jnp.dot(wide, in_all[...], preferred_element_type=jnp.float32) * scale
        chan[at, :] = value
        first = value.astype(jnp.bfloat16)
        high[at, :] = first
        low_part[at, :] = (value - first.astype(jnp.float32)).astype(jnp.bfloat16)
        return 0

    lax.fori_loop(0, 4, channel_rows, 0)

    def extent(position, length):
        upper = jnp.minimum(position + above, length)
        return upper - jnp.maximum(position - below, 0)

    def pool_rows(i, _):
        at = pl.ds(pl.multiple_of(i * chunk, 16), chunk)
        inside = mask[at, :]
        total = jnp.dot(inside, high[...], preferred_element_type=jnp.float32) + jnp.dot(
            inside, low_part[...], preferred_element_type=jnp.float32
        )
        cell = i * chunk + lax.broadcasted_iota(jnp.int32, (chunk, block), 0)
        cells = extent(cell // GRID_W, rows // GRID_W) * extent(cell % GRID_W, GRID_W)
        pooled[at, :] = (total / cells.astype(jnp.float32) - chan[at, :]).astype(jnp.bfloat16)
        return 0

    lax.fori_loop(0, 4, pool_rows, 0)

    g_out.rows_y()

    for k in range(4):
        part = pooled[piece(k), :]
        for dx in (0, 1):
            for dc in (0, 1):
                target = mix_own if dc == 0 else mix_cs
                for side in (0, 1):
                    j = column_of(dx, dc) * 2 + side
                    term = jnp.dot(part, out_all[j], preferred_element_type=jnp.float32)
                    target[k, dx, :, side * block:(side + 1) * block] = term.astype(jnp.bfloat16)
        mail.send(mix_cs.at[k], mix_cr.at[k], m_send.at[0, k], m_recv.at[0, k], p.to_c)

    def both(k, dx):
        return mix_own[k, dx].astype(jnp.float32) + mix_cr[k, dx].astype(jnp.float32)

    for k in range(4):
        mail.arrived(mix_cr.at[k], m_recv.at[0, k])
        mix_xs[k] = both(k, 1).astype(jnp.bfloat16)
        mail.send(mix_xs.at[k], mix_xr.at[k], m_send.at[1, k], m_recv.at[1, k], p.to_x)

    def res_at(dz, column, k):
        return res.at[(p.zl + dz) % 2, piece(k), lanes(column * cols, cols)]

    def res_send(dz, column, k, lane, device):
        here = res_at(dz, column, k)
        sem = ((p.zl + dz) % 2) * 4 + column
        mail.send(here, here, r_send.at[lane, k], r_recv.at[sem, k], device)

    def res_wait(dz, column, k):
        sem = ((p.zl + dz) % 2) * 4 + column
        mail.arrived(res_at(dz, column, k), r_recv.at[sem, k])

    for k in range(4):
        mail.arrived(mix_xr.at[k], m_recv.at[1, k])
        mine = lanes(p.column * cols, cols)
        total = both(k, 0) + mix_xr[k].astype(jnp.float32)
        total = total + tokens[piece(k), mine].astype(jnp.float32)
        res[p.zl, piece(k), mine] = total.astype(jnp.bfloat16)
        res_send(0, p.column, k, 0, p.to_x)
        res_send(0, p.column, k, 1, p.to_zl)
        res_send(0, p.column, k, 2, p.to_c)
        if k > 1:
            g_gu[k - 2].on_zl()
    g_dn.start_zl(dn_other)
    g_dn.start_zh(kept(4)(p.index))

    across = column_of(1, 0)
    for k in range(4):
        res_wait(0, across, k)
        res_send(0, across, k, 5, p.to_c)
        res_wait(1, p.column, k)
        res_send(1, p.column, k, 3, p.to_x)
        res_send(1, p.column, k, 4, p.to_c)
        g_gu[k % 2].on_zh(k // 2)
    for k in range(4):
        for dx in (0, 1):
            res_wait(0, column_of(dx, 1), k)
    for q in (0, 1):
        g_gu[q].rows_y()

    def hidden_rows(dz):
        def body(i, _):
            at = pl.ds(pl.multiple_of(i * chunk, 16), chunk)
            z = (p.zl + dz) % 2
            wide, scale = normed(res[z, at, :].astype(jnp.float32), gain_ffn)
            for q in (0, 1):
                value = jnp.dot(wide, gu_all[q], preferred_element_type=jnp.float32) * scale
                gate, up = value[:, :half], value[:, half:]
                unit = gate / (1.0 + jnp.exp(-gate)) * up
                hid[z, at, q * half:(q + 1) * half] = unit.astype(jnp.bfloat16)
            return 0

        return body

    lax.fori_loop(0, 4, hidden_rows(0), 0)
    g_dn.on_zl()
    for k in range(4):
        res_wait(1, across, k)
        res_send(1, across, k, 6, p.to_c)
    for k in range(4):
        for dx in (0, 1):
            res_wait(1, column_of(dx, 1), k)
    lax.fori_loop(0, 4, hidden_rows(1), 0)
    g_dn.on_zh(0)
    g_dn.on_zh(1)

    mail.settle(passed)

    def sum_own(u, dx):
        return tokens.at[pl.ds((u % 2) * tall, tall), pl.ds((u // 2 * 2 + dx) * block, block)]

    def unit(dy, dz, k):
        return dy * 4 + dz * 2 + k

    def pair(u, dx):
        return sum_own(u, dx)[...].astype(jnp.float32) + sum_cr[u, dx].astype(jnp.float32)

    def x_send_at(n):
        mail.send(sum_xs.at[n], sum_xr.at[n], x_send.at[n], x_recv.at[n], p.to_x)

    def z_send_at(n):
        mail.send(sum_zs.at[n], sum_zr.at[n], z_send.at[n], z_recv.at[n], p.to_zl)

    def stage_core(dy, dz, k):
        u = unit(dy, dz, k)
        part = hid[(p.zl + dz) % 2, pl.ds(k * tall, tall), :]
        for dc in (1, 0):
            for dx in (0, 1):
                j = column_of(dx, dc) * 2 + (p.y + dy) % 2
                term = jnp.dot(part, dn_all[j], preferred_element_type=jnp.float32)
                if dc == 0:
                    sum_own(u, dx)[...] = term.astype(jnp.bfloat16)
                else:
                    sum_cs[u, dx] = term.astype(jnp.bfloat16)
            if dc:
                mail.send(sum_cs.at[u], sum_cr.at[u], c_send.at[u], c_recv.at[u], p.to_c)

    def stage_first(dy, dz, k):
        u = unit(dy, dz, k)
        mail.arrived(sum_cr.at[u], c_recv.at[u])
        if k == 0:
            n = dy * 3 + dz
            sum_xs[n] = pair(u, 1).astype(jnp.bfloat16)
            x_send_at(n)
        elif dz == 1:
            for dx in (1, 0):
                n = dy * 3 + dx
                sum_zs[n] = pair(u, dx).astype(jnp.bfloat16)
                z_send_at(n)

    def stage_second(dy):
        n = dy * 3
        mail.arrived(sum_xr.at[n + 1], x_recv.at[n + 1])
        total = pair(unit(dy, 1, 0), 0) + sum_xr[n + 1].astype(jnp.float32)
        sum_zs[n + 2] = total.astype(jnp.bfloat16)
        z_send_at(n + 2)
        mail.arrived(sum_zr.at[n + 1], z_recv.at[n + 1])
        total = pair(unit(dy, 0, 1), 1) + sum_zr[n + 1].astype(jnp.float32)
        sum_xs[n + 2] = total.astype(jnp.bfloat16)
        x_send_at(n + 2)

    def stage_last(dy):
        n = dy * 3
        side = (p.y + dy) % 2 * block
        for k in (0, 1):
            first, second = (n, n + 2) if k == 0 else (n + 2, n)
            mail.arrived(sum_xr.at[first], x_recv.at[first])
            mail.arrived(sum_zr.at[second], z_recv.at[second])
            total = pair(unit(dy, 0, k), 0)
            total = total + sum_xr[first].astype(jnp.float32) + sum_zr[second].astype(jnp.float32)
            at = pl.ds(k * tall, tall)
            total = total + res[p.zl, at, lanes(p.column * cols + side, block)].astype(jnp.float32)
            done[at, lanes(side, block)] = total.astype(jnp.bfloat16)

    order = [(1, 0), (1, 1), (0, 0), (0, 1)]
    for dy in (0, 1):
        if dy:
            g_dn.rows_y()
        for n, (dz, k) in enumerate(order):
            stage_core(dy, dz, k)
            if n:
                stage_first(dy, *order[n - 1])
        stage_first(dy, *order[3])
    for dy in (0, 1):
        stage_second(dy)
    for dy in (0, 1):
        stage_last(dy)
    copy = pltpu.make_async_copy(done, out, local_sem.at[0])
    copy.start()
    mail.close()
    copy.wait()


def paired(mesh):
    fs, tp = mesh.shape["fs"], mesh.shape["tp"]

    def local(
        tokens,
        mix_gain,
        in_weight,
        in_scale,
        out_weight,
        out_scale,
        ffn_gain,
        gate_weight,
        gate_scale,
        up_weight,
        up_scale,
        down_weight,
        down_scale,
    ):
        rows, cols = tokens.shape
        depth, block = in_weight.shape
        wide = gate_weight.shape[1]
        features = cols * tp
        low_type = jnp.bfloat16
        tall = rows // 2
        buffers = [
            ((rows, features), low_type),
            ((2, rows, features), low_type),
            ((features, block), low_type),
            ((fs, block, block), low_type),
            ((2, features, wide // 2), low_type),
            ((fs, wide // 2, block), low_type),
            ((2, rows, wide // 2), low_type),
            ((rows, rows), low_type),
            ((rows, block), jnp.float32),
            ((rows, block), low_type),
            ((rows, block), low_type),
            ((rows, block), low_type),
            ((4, 2, rows // 4, cols), low_type),
            ((4, 2, rows // 4, cols), low_type),
            ((4, 2, rows // 4, cols), low_type),
            ((4, rows // 4, cols), low_type),
            ((4, rows // 4, cols), low_type),
            ((8, 2, tall, block), low_type),
            ((8, 2, tall, block), low_type),
            ((6, tall, block), low_type),
            ((6, tall, block), low_type),
            ((6, tall, block), low_type),
            ((6, tall, block), low_type),
            ((rows, cols), low_type),
            (in_weight.shape, jnp.float32),
            (out_weight.shape, jnp.float32),
            (gate_weight.shape, jnp.float32),
            (up_weight.shape, jnp.float32),
            (down_weight.shape, jnp.float32),
            ((2, depth, wide // 2), low_type),
            ((wide // 2, block), low_type),
        ]
        semaphores = [(6,), (5, 7), (5, fs), (3, 4), (tp, 4), (7, 4), (2 * tp, 4), (2, 4), (2, 4)]
        semaphores += [(8,), (8,), (6,), (6,), (6,), (6,)]
        anywhere = pl.BlockSpec(memory_space=pl.ANY)
        inside = pl.BlockSpec(memory_space=pltpu.VMEM)
        vectors = (mix_gain, ffn_gain, in_scale, out_scale, gate_scale, up_scale, down_scale)
        return pl.pallas_call(
            fused,
            out_shape=jax.ShapeDtypeStruct((rows, cols), low_type),
            in_specs=[anywhere] * 6 + [inside] * len(vectors),
            out_specs=anywhere,
            scratch_shapes=[pltpu.VMEM(shape, kind) for shape, kind in buffers]
            + [pltpu.SemaphoreType.DMA(shape) for shape in semaphores],
            compiler_params=pltpu.CompilerParams(
                collective_id=0, has_side_effects=True, vmem_limit_bytes=67043328
            ),
        )(
            tokens,
            in_weight,
            out_weight,
            gate_weight,
            up_weight,
            down_weight,
            *vectors,
        )

    return jax.shard_map(
        local, mesh=mesh, in_specs=IN_SPECS, out_specs=P("fs", "tp"), check_vma=False
    )


def solution(mesh):
    fs, tp = mesh.shape["fs"], mesh.shape["tp"]
    xs = max(tp // 2, 1)
    return paired(mesh) if (xs, fs // xs) == (2, 4) else general(mesh)
```

```python
import jax
import jax.numpy as jnp
from jax import lax
from jax.experimental import pallas as pl
from jax.experimental.pallas import tpu as pltpu
from jax.sharding import PartitionSpec as P

GROUPS = 4
GRID_W = 64
GC = 256
WINDOWS = (2, 4, 8, 16)
EPSILON = 1e-06


IN_SPECS = (
    P("fs", "tp"),
    P(),
    P("fs", "tp"),
    P("tp"),
    P("tp", "fs"),
    P("fs"),
    P(),
    P("fs", "tp"),
    P("tp"),
    P("fs", "tp"),
    P("tp"),
    P("tp", "fs"),
    P("fs"),
)


def box_matrix(length, window):
    position = jnp.arange(length, dtype=jnp.int32)
    lower_end = jnp.clip(position - window // 2, 0, length)
    upper_end = jnp.clip(position + (window - window // 2), 0, length)
    inside = (position[None, :] >= lower_end[:, None]) & (position[None, :] < upper_end[:, None])
    return inside.astype(jnp.float32) / (upper_end - lower_end).astype(jnp.float32)[:, None]


def smooth(lattice, window):
    across = jnp.einsum(
        "jk,akc->ajc", box_matrix(GRID_W, window), lattice, precision=lax.Precision.HIGHEST
    )
    return jnp.einsum(
        "ab,bjc->ajc",
        box_matrix(lattice.shape[0], window),
        across,
        precision=lax.Precision.HIGHEST,
    )


def pooled_differences(channels, channel_offset):
    tokens_here, extent = channels.shape
    lattice = channels.reshape(tokens_here // GRID_W, GRID_W, extent)
    if GC % extent == 0:
        result = smooth(lattice, jnp.asarray(WINDOWS, jnp.int32)[channel_offset // GC])
    else:
        group_of = (channel_offset + jnp.arange(extent, dtype=jnp.int32)) // GC
        result = jnp.zeros_like(lattice)
        for group in range(GROUPS):
            result = jnp.where(
                (group_of == group)[None, None, :], smooth(lattice, WINDOWS[group]), result
            )
    return (result - lattice).reshape(tokens_here, extent).astype(jnp.bfloat16)


class Grid:
    def __init__(self, fs, tp):
        self.ys = max(tp // 2, 1)
        self.zs = fs // self.ys
        index = lax.axis_index("fs")
        self.z, self.y = index // self.ys, index % self.ys

    def gather(self, block):
        rows = []
        for s in range(self.zs):
            pairs = [
                (z * self.ys + y, (z + s) % self.zs * self.ys + y)
                for z in range(self.zs)
                for y in range(self.ys)
            ]
            rows.append(lax.ppermute(block, "fs", pairs) if s else block)
        found = []
        for s, row in enumerate(rows):
            for t in range(self.ys):
                pairs = [
                    (z * self.ys + y, z * self.ys + (y + t) % self.ys)
                    for z in range(self.zs)
                    for y in range(self.ys)
                ]
                item = lax.ppermute(row, "fs", pairs) if t else row
                index = lax.rem(self.z - s + self.zs, self.zs) * self.ys + lax.rem(
                    self.y - t + self.ys, self.ys
                )
                found.append((index, item))
        return found


def stack(pieces):
    shape = (len(pieces),) + pieces[0][1].shape
    result = jnp.zeros(shape, pieces[0][1].dtype)
    for index, item in pieces:
        result = lax.dynamic_update_index_in_dim(result, item, index, 0)
    return result


def rows_of(pieces):
    whole = stack(pieces)
    return whole.reshape(whole.shape[0] * whole.shape[1], whole.shape[2])


def fold_rows(features, gain, weights):
    widened = lax.all_gather(features, "tp", axis=1, tiled=True)
    widened = widened.astype(jnp.float32)
    inverse_rms = lax.rsqrt(jnp.mean(widened * widened, axis=1) + EPSILON)[:, None]
    scaled = (widened * gain).astype(jnp.bfloat16)
    return tuple(
        jnp.dot(scaled, weight, preferred_element_type=jnp.float32) * inverse_rms
        for weight in weights
    )


def column_product(hidden, pieces):
    terms = stack(
        [
            (index, jnp.dot(hidden, item, preferred_element_type=jnp.float32).astype(jnp.bfloat16))
            for index, item in pieces
        ]
    )
    mine = lax.psum_scatter(terms, "tp", scatter_dimension=0, tiled=True)
    return mine.transpose(1, 0, 2).reshape(hidden.shape[0], -1).astype(jnp.float32)


def low(weight, scale=None):
    weight = weight.astype(jnp.bfloat16)
    if scale is None:
        return weight
    return (weight.astype(jnp.float32) * scale).astype(jnp.bfloat16)


def general(mesh):
    fs, tp = mesh.shape["fs"], mesh.shape["tp"]

    def layer(
        tokens,
        mix_gain,
        in_weight,
        in_scale,
        out_weight,
        out_scale,
        ffn_gain,
        gate_weight,
        gate_scale,
        up_weight,
        up_scale,
        down_weight,
        down_scale,
    ):
        grid = Grid(fs, tp)
        wide = gate_weight.shape[1]
        both_pieces = grid.gather(jnp.concatenate([low(gate_weight), low(up_weight)], axis=1))
        down_pieces = grid.gather(low(down_weight, down_scale))
        small = lax.all_gather(
            jnp.stack([low(in_weight), low(out_weight, out_scale)]), "fs", axis=0
        )
        in_full = small[:, 0].reshape(-1, in_weight.shape[1])
        out_pieces = [(j, small[j, 1]) for j in range(fs)]
        (channels,) = fold_rows(tokens, mix_gain, (in_full,))
        channels = channels * in_scale
        pooled = pooled_differences(channels, lax.axis_index("tp") * channels.shape[1])
        mixed = column_product(pooled, out_pieces)
        residual = (tokens.astype(jnp.float32) + mixed).astype(jnp.bfloat16)
        (both,) = fold_rows(residual, ffn_gain, (rows_of(both_pieces),))
        gate_value = both[:, :wide] * gate_scale
        up_value = both[:, wide:] * up_scale
        hidden = (jax.nn.silu(gate_value) * up_value).astype(jnp.bfloat16)
        channel_out = column_product(hidden, down_pieces)
        return (residual.astype(jnp.float32) + channel_out).astype(jnp.bfloat16)

    return jax.shard_map(
        layer, mesh=mesh, in_specs=IN_SPECS, out_specs=P("fs", "tp"), check_vma=False
    )


class Place:
    def __init__(self):
        index, column = lax.axis_index("fs"), lax.axis_index("tp")
        z, self.y = index // 2, index % 2
        self.zh, self.zl = z // 2, z % 2
        self.x, self.c = column // 2, column % 2
        self.index, self.column = index, column
        self.to_x = {"tp": (1 - self.x) * 2 + self.c}
        self.to_c = {"tp": self.x * 2 + 1 - self.c}
        self.to_y = {"fs": z * 2 + 1 - self.y}
        self.to_zl = {"fs": (self.zh * 2 + 1 - self.zl) * 2 + self.y}
        self.to_zh = {"fs": ((1 - self.zh) * 2 + self.zl) * 2 + self.y}

    def slot(self, dh, dl, dy):
        zh, zl, y = (self.zh + dh) % 2, (self.zl + dl) % 2, (self.y + dy) % 2
        return (zh * 2 + zl) * 2 + y


class Mail:
    def __init__(self):
        self.started = []

    def send(self, source, target, send_sem, recv_sem, device):
        copy = pltpu.make_async_remote_copy(
            src_ref=source,
            dst_ref=target,
            send_sem=send_sem,
            recv_sem=recv_sem,
            device_id=device,
            device_id_type=pl.DeviceIdType.MESH,
        )
        copy.start()
        self.started.append(copy)
        return copy

    def arrived(self, target, recv_sem):
        pltpu.make_async_copy(target, target, recv_sem).wait()

    def settle(self, copies):
        for copy in copies:
            copy.wait_send()
        self.started = [copy for copy in self.started if all(copy is not c for c in copies)]

    def close(self):
        self.settle(self.started)


class Gather:
    def __init__(self, mail, place, kind, target, sends, recvs):
        self.mail, self.place, self.kind = mail, place, kind
        self.target, self.sends, self.recvs = target, sends, recvs
        self.count = 0

    def pass_on(self, source, slot, device):
        self.mail.send(
            source,
            self.target(slot),
            self.sends.at[self.kind, self.count],
            self.recvs.at[self.kind, slot],
            device,
        )
        self.count += 1

    def forward(self, slot, *devices):
        self.mail.arrived(self.target(slot), self.recvs.at[self.kind, slot])
        for device in devices:
            self.pass_on(self.target(slot), slot, device)

    def rows_y(self):
        for dh, dl in ((0, 0), (0, 1), (1, 0), (1, 1)):
            self.forward(self.place.slot(dh, dl, 1))


class WholeGather(Gather):
    def start(self, own):
        p = self.place
        self.pass_on(own, p.index, p.to_zh)
        self.pass_on(own, p.index, p.to_zl)
        self.pass_on(own, p.index, p.to_y)

    def on_zh(self):
        p = self.place
        self.forward(p.slot(1, 0, 0), p.to_zl, p.to_y)

    def on_zl(self):
        p = self.place
        self.forward(p.slot(0, 1, 0), p.to_y)
        self.forward(p.slot(1, 1, 0), p.to_y)


class HalfGather(Gather):
    def start_zl(self, other):
        self.pass_on(other, self.place.index, self.place.to_zl)

    def start_zh(self, own):
        self.pass_on(own, self.place.index, self.place.to_zh)

    def start_y(self, own):
        self.pass_on(own, self.place.index, self.place.to_y)

    def on_zl(self):
        p = self.place
        self.forward(p.slot(0, 1, 0), p.to_zh, p.to_y)

    def on_zh(self, dl):
        p = self.place
        self.forward(p.slot(1, dl, 0), p.to_y)


def lanes(start, size):
    return pl.ds(pl.multiple_of(start, 128), size)


def fused(
    tok, w_in, w_out, w_gate, w_up, w_down,
    gain_mix, gain_ffn, s_in, s_out, s_gate, s_up, s_down, out,
    tokens, res, in_all, out_all, gu_all, dn_all, hid, mask, chan, high, low_part, pooled,
    mix_cs, mix_cr, mix_own, mix_xs, mix_xr,
    sum_cs, sum_cr, sum_xs, sum_xr, sum_zs, sum_zr, done,
    f_in, f_out, f_gate, f_up, f_down, gu_other, dn_other,
    local_sem, w_send, w_recv, t_send, t_recv, r_send, r_recv, m_send, m_recv,
    c_send, c_recv, x_send, x_recv, z_send, z_recv,
):
    rows, features = tokens.shape
    cols = tok.shape[1]
    block = w_in.shape[0]
    unit_hidden = dn_all.shape[1]
    half = gu_all.shape[2] // 2
    chunk = rows // 4
    tall = rows // 2
    p, mail = Place(), Mail()

    def kept(kind):
        return {
            0: lambda j: in_all.at[pl.ds(pl.multiple_of(j * block, 16), block), :],
            1: lambda j: out_all.at[j],
            2: lambda j: gu_all.at[0, pl.ds(pl.multiple_of(j * block, 16), block), :],
            3: lambda j: gu_all.at[1, pl.ds(pl.multiple_of(j * block, 16), block), :],
            4: lambda j: dn_all.at[j],
        }[kind]

    g_in, g_out = (WholeGather(mail, p, k, kept(k), w_send, w_recv) for k in (0, 1))
    g_gu = [HalfGather(mail, p, 2 + q, kept(2 + q), w_send, w_recv) for q in (0, 1)]
    g_dn = HalfGather(mail, p, 4, kept(4), w_send, w_recv)

    def piece(k):
        return pl.ds(k * chunk, chunk)

    def column_of(dx, dc):
        return ((p.x + dx) % 2) * 2 + (p.c + dc) % 2

    copies = [
        pltpu.make_async_copy(source, target, local_sem.at[n])
        for n, (source, target) in enumerate((
            (w_in, f_in),
            (w_out, f_out),
            (tok, tokens.at[:, lanes(p.column * cols, cols)]),
            (w_gate, f_gate),
            (w_up, f_up),
            (w_down, f_down),
        ))
    ]
    for copy in copies:
        copy.start()
    barrier = pltpu.get_barrier_semaphore()
    for device in (p.to_c, p.to_x, p.to_y, p.to_zl, p.to_zh):
        pl.semaphore_signal(
            barrier, inc=1, device_id=device, device_id_type=pl.DeviceIdType.MESH
        )
    pl.semaphore_wait(barrier, 5)
    for k in range(4):
        own = tok.at[piece(k), :]
        at = tokens.at[piece(k), lanes(p.column * cols, cols)]
        mail.send(own, at, t_send.at[0, k], t_recv.at[p.column, k], p.to_x)
        mail.send(own, at, t_send.at[1, k], t_recv.at[p.column, k], p.to_c)

    def rounded(weight, scale):
        weight = weight.astype(jnp.bfloat16).astype(jnp.float32)
        return (weight * scale[None, :]).astype(jnp.bfloat16)

    copies[0].wait()
    kept(0)(p.index)[...] = rounded(f_in[...], s_in[...])
    g_in.start(kept(0)(p.index))
    copies[1].wait()
    kept(1)(p.index)[...] = rounded(f_out[...], s_out[...])
    g_out.start(kept(1)(p.index))
    for copy in copies[3:]:
        copy.wait()
    for q in (0, 1):
        for own in (True, False):
            target = kept(2 + q)(p.index) if own else gu_other.at[q]
            at = lanes(((p.zl if own else 1 - p.zl) * 2 + q) * half, half)
            target[:, :half] = rounded(f_gate[:, at], s_gate[at])
            target[:, half:] = rounded(f_up[:, at], s_up[at])
    for own in (True, False):
        target = kept(4)(p.index) if own else dn_other
        at = (p.zl if own else 1 - p.zl) * unit_hidden
        at = pl.ds(pl.multiple_of(at, 16), unit_hidden)
        target[...] = rounded(f_down[at, :], s_down[...])

    window = lax.shift_left(2, p.column * block // GC)
    below = window // 2
    above = window - below

    def mask_rows(i, _):
        cell = i * chunk // 2 + lax.broadcasted_iota(jnp.int32, (chunk // 2, rows), 0)
        other = lax.broadcasted_iota(jnp.int32, (chunk // 2, rows), 1)
        dr = other // GRID_W - cell // GRID_W
        dc = other % GRID_W - cell % GRID_W
        inside = (dr >= -below) & (dr < above) & (dc >= -below) & (dc < above)
        at = pl.ds(pl.multiple_of(i * (chunk // 2), 16), chunk // 2)
        mask[at, :] = jnp.where(inside, 1.0, 0.0).astype(jnp.bfloat16)
        return 0

    lax.fori_loop(0, 8, mask_rows, 0)

    g_in.on_zh()
    g_out.on_zh()
    g_in.on_zl()
    g_out.on_zl()
    for q in (0, 1):
        g_gu[q].start_zl(gu_other.at[q])
    for q in (0, 1):
        g_gu[q].start_zh(kept(2 + q)(p.index))
    for q in (0, 1):
        g_gu[q].start_y(kept(2 + q)(p.index))
    g_dn.start_y(kept(4)(p.index))

    def token_at(column, k):
        return tokens.at[piece(k), lanes(column * cols, cols)]

    passed = []
    for k in range(4):
        column = column_of(1, 0)
        here = token_at(column, k)
        mail.arrived(here, t_recv.at[column, k])
        passed.append(mail.send(here, here, t_send.at[2, k], t_recv.at[column, k], p.to_c))
    copies[2].wait()
    for dx in (0, 1):
        for k in range(4):
            column = column_of(dx, 1)
            mail.arrived(token_at(column, k), t_recv.at[column, k])
    g_in.rows_y()

    def normed(wide, gain):
        square = wide * wide
        scale = lax.rsqrt(jnp.sum(square, axis=1, keepdims=True) / features + EPSILON)
        return (wide * gain[...][None, :]).astype(jnp.bfloat16), scale

    def channel_rows(i, _):
        at = pl.ds(pl.multiple_of(i * chunk, 16), chunk)
        wide, scale = normed(tokens[at, :].astype(jnp.float32), gain_mix)
        value = jnp.dot(wide, in_all[...], preferred_element_type=jnp.float32) * scale
        chan[at, :] = value
        first = value.astype(jnp.bfloat16)
        high[at, :] = first
        low_part[at, :] = (value - first.astype(jnp.float32)).astype(jnp.bfloat16)
        return 0

    lax.fori_loop(0, 4, channel_rows, 0)

    def extent(position, length):
        upper = jnp.minimum(position + above, length)
        return upper - jnp.maximum(position - below, 0)

    def pool_rows(i, _):
        at = pl.ds(pl.multiple_of(i * chunk, 16), chunk)
        inside = mask[at, :]
        total = jnp.dot(inside, high[...], preferred_element_type=jnp.float32) + jnp.dot(
            inside, low_part[...], preferred_element_type=jnp.float32
        )
        cell = i * chunk + lax.broadcasted_iota(jnp.int32, (chunk, block), 0)
        cells = extent(cell // GRID_W, rows // GRID_W) * extent(cell % GRID_W, GRID_W)
        pooled[at, :] = (total / cells.astype(jnp.float32) - chan[at, :]).astype(jnp.bfloat16)
        return 0

    lax.fori_loop(0, 4, pool_rows, 0)

    g_out.rows_y()

    for k in range(4):
        part = pooled[piece(k), :]
        for dx in (0, 1):
            for dc in (0, 1):
                target = mix_own if dc == 0 else mix_cs
                for side in (0, 1):
                    j = column_of(dx, dc) * 2 + side
                    term = jnp.dot(part, out_all[j], preferred_element_type=jnp.float32)
                    target[k, dx, :, side * block:(side + 1) * block] = term.astype(jnp.bfloat16)
        mail.send(mix_cs.at[k], mix_cr.at[k], m_send.at[0, k], m_recv.at[0, k], p.to_c)

    def both(k, dx):
        return mix_own[k, dx].astype(jnp.float32) + mix_cr[k, dx].astype(jnp.float32)

    for k in range(4):
        mail.arrived(mix_cr.at[k], m_recv.at[0, k])
        mix_xs[k] = both(k, 1).astype(jnp.bfloat16)
        mail.send(mix_xs.at[k], mix_xr.at[k], m_send.at[1, k], m_recv.at[1, k], p.to_x)

    def res_at(dz, column, k):
        return res.at[(p.zl + dz) % 2, piece(k), lanes(column * cols, cols)]

    def res_send(dz, column, k, lane, device):
        here = res_at(dz, column, k)
        sem = ((p.zl + dz) % 2) * 4 + column
        mail.send(here, here, r_send.at[lane, k], r_recv.at[sem, k], device)

    def res_wait(dz, column, k):
        sem = ((p.zl + dz) % 2) * 4 + column
        mail.arrived(res_at(dz, column, k), r_recv.at[sem, k])

    for k in range(4):
        mail.arrived(mix_xr.at[k], m_recv.at[1, k])
        mine = lanes(p.column * cols, cols)
        total = both(k, 0) + mix_xr[k].astype(jnp.float32)
        total = total + tokens[piece(k), mine].astype(jnp.float32)
        res[p.zl, piece(k), mine] = total.astype(jnp.bfloat16)
        res_send(0, p.column, k, 0, p.to_x)
        res_send(0, p.column, k, 1, p.to_zl)
        res_send(0, p.column, k, 2, p.to_c)
        if k > 1:
            g_gu[k - 2].on_zl()
    g_dn.start_zl(dn_other)
    g_dn.start_zh(kept(4)(p.index))

    across = column_of(1, 0)

    def on_x(k):
        res_wait(0, across, k)
        res_send(0, across, k, 5, p.to_c)

    def on_z(k):
        res_wait(1, p.column, k)
        res_send(1, p.column, k, 3, p.to_x)
        res_send(1, p.column, k, 4, p.to_c)

    def on_both(k):
        res_wait(1, across, k)
        res_send(1, across, k, 6, p.to_c)

    on_x(0)
    g_gu[0].on_zh(0)
    on_x(1)
    g_gu[1].on_zh(0)
    on_x(2)
    on_z(0)
    on_x(3)
    on_z(1)
    g_gu[0].on_zh(1)
    on_z(2)
    g_gu[1].on_zh(1)
    on_z(3)
    on_both(0)
    on_both(1)
    for k in range(4):
        for dx in (0, 1):
            res_wait(0, column_of(dx, 1), k)
    for q in (0, 1):
        g_gu[q].rows_y()

    def hidden_rows(dz):
        def body(i, _):
            at = pl.ds(pl.multiple_of(i * chunk, 16), chunk)
            z = (p.zl + dz) % 2
            wide, scale = normed(res[z, at, :].astype(jnp.float32), gain_ffn)
            for q in (0, 1):
                value = jnp.dot(wide, gu_all[q], preferred_element_type=jnp.float32) * scale
                gate, up = value[:, :half], value[:, half:]
                unit = gate / (1.0 + jnp.exp(-gate)) * up
                hid[z, at, q * half:(q + 1) * half] = unit.astype(jnp.bfloat16)
            return 0

        return body

    lax.fori_loop(0, 1, hidden_rows(0), 0)
    g_dn.on_zl()
    on_both(2)
    lax.fori_loop(1, 3, hidden_rows(0), 0)
    on_both(3)
    lax.fori_loop(3, 4, hidden_rows(0), 0)
    g_dn.on_zh(0)
    for k in range(4):
        for dx in (0, 1):
            res_wait(1, column_of(dx, 1), k)
    lax.fori_loop(0, 4, hidden_rows(1), 0)
    g_dn.on_zh(1)

    mail.settle(passed)

    def sum_own(u, dx):
        return tokens.at[pl.ds((u % 2) * tall, tall), pl.ds((u // 2 * 2 + dx) * block, block)]

    def unit(dy, dz, k):
        return dy * 4 + dz * 2 + k

    def pair(u, dx):
        return sum_own(u, dx)[...].astype(jnp.float32) + sum_cr[u, dx].astype(jnp.float32)

    def x_send_at(n):
        mail.send(sum_xs.at[n], sum_xr.at[n], x_send.at[n], x_recv.at[n], p.to_x)

    def z_send_at(n):
        mail.send(sum_zs.at[n], sum_zr.at[n], z_send.at[n], z_recv.at[n], p.to_zl)

    def stage_core(dy, dz, k):
        u = unit(dy, dz, k)
        part = hid[(p.zl + dz) % 2, pl.ds(k * tall, tall), :]
        for dc in (1, 0):
            for dx in (0, 1):
                j = column_of(dx, dc) * 2 + (p.y + dy) % 2
                term = jnp.dot(part, dn_all[j], preferred_element_type=jnp.float32)
                if dc == 0:
                    sum_own(u, dx)[...] = term.astype(jnp.bfloat16)
                else:
                    sum_cs[u, dx] = term.astype(jnp.bfloat16)
            if dc:
                mail.send(sum_cs.at[u], sum_cr.at[u], c_send.at[u], c_recv.at[u], p.to_c)

    def stage_first(dy, dz, k):
        u = unit(dy, dz, k)
        mail.arrived(sum_cr.at[u], c_recv.at[u])
        if k == 0:
            n = dy * 3 + dz
            sum_xs[n] = pair(u, 1).astype(jnp.bfloat16)
            x_send_at(n)
        elif dz == 1:
            for dx in (1, 0):
                n = dy * 3 + dx
                sum_zs[n] = pair(u, dx).astype(jnp.bfloat16)
                z_send_at(n)

    def stage_second(dy):
        n = dy * 3
        mail.arrived(sum_xr.at[n + 1], x_recv.at[n + 1])
        total = pair(unit(dy, 1, 0), 0) + sum_xr[n + 1].astype(jnp.float32)
        sum_zs[n + 2] = total.astype(jnp.bfloat16)
        z_send_at(n + 2)
        mail.arrived(sum_zr.at[n + 1], z_recv.at[n + 1])
        total = pair(unit(dy, 0, 1), 1) + sum_zr[n + 1].astype(jnp.float32)
        sum_xs[n + 2] = total.astype(jnp.bfloat16)
        x_send_at(n + 2)

    results = []

    def stage_last(dy):
        n = dy * 3
        side = (p.y + dy) % 2 * block
        for k in (0, 1):
            first, second = (n, n + 2) if k == 0 else (n + 2, n)
            mail.arrived(sum_xr.at[first], x_recv.at[first])
            mail.arrived(sum_zr.at[second], z_recv.at[second])
            total = pair(unit(dy, 0, k), 0)
            total = total + sum_xr[first].astype(jnp.float32) + sum_zr[second].astype(jnp.float32)
            at = pl.ds(k * tall, tall)
            total = total + res[p.zl, at, lanes(p.column * cols + side, block)].astype(jnp.float32)
            here = (at, lanes(side, block))
            done[here] = total.astype(jnp.bfloat16)
            copy = pltpu.make_async_copy(done.at[here], out.at[here], local_sem.at[dy * 2 + k])
            copy.start()
            results.append(copy)

    order = [(1, 0), (1, 1), (0, 0), (0, 1)]
    for dy in (0, 1):
        if dy:
            g_dn.rows_y()
        for n, (dz, k) in enumerate(order):
            stage_core(dy, dz, k)
            if n > 1:
                stage_first(dy, *order[n - 2])
        for n in (2, 3):
            stage_first(dy, *order[n])
    for dy in (0, 1):
        stage_second(dy)
    for dy in (0, 1):
        stage_last(dy)
    mail.close()
    for copy in results:
        copy.wait()


def paired(mesh):
    fs, tp = mesh.shape["fs"], mesh.shape["tp"]

    def local(
        tokens,
        mix_gain,
        in_weight,
        in_scale,
        out_weight,
        out_scale,
        ffn_gain,
        gate_weight,
        gate_scale,
        up_weight,
        up_scale,
        down_weight,
        down_scale,
    ):
        rows, cols = tokens.shape
        depth, block = in_weight.shape
        wide = gate_weight.shape[1]
        features = cols * tp
        low_type = jnp.bfloat16
        tall = rows // 2
        buffers = [
            ((rows, features), low_type),
            ((2, rows, features), low_type),
            ((features, block), low_type),
            ((fs, block, block), low_type),
            ((2, features, wide // 2), low_type),
            ((fs, wide // 2, block), low_type),
            ((2, rows, wide // 2), low_type),
            ((rows, rows), low_type),
            ((rows, block), jnp.float32),
            ((rows, block), low_type),
            ((rows, block), low_type),
            ((rows, block), low_type),
            ((4, 2, rows // 4, cols), low_type),
            ((4, 2, rows // 4, cols), low_type),
            ((4, 2, rows // 4, cols), low_type),
            ((4, rows // 4, cols), low_type),
            ((4, rows // 4, cols), low_type),
            ((8, 2, tall, block), low_type),
            ((8, 2, tall, block), low_type),
            ((6, tall, block), low_type),
            ((6, tall, block), low_type),
            ((6, tall, block), low_type),
            ((6, tall, block), low_type),
            ((rows, cols), low_type),
            (in_weight.shape, jnp.float32),
            (out_weight.shape, jnp.float32),
            (gate_weight.shape, jnp.float32),
            (up_weight.shape, jnp.float32),
            (down_weight.shape, jnp.float32),
            ((2, depth, wide // 2), low_type),
            ((wide // 2, block), low_type),
        ]
        semaphores = [(6,), (5, 7), (5, fs), (3, 4), (tp, 4), (7, 4), (2 * tp, 4), (2, 4), (2, 4)]
        semaphores += [(8,), (8,), (6,), (6,), (6,), (6,)]
        anywhere = pl.BlockSpec(memory_space=pl.ANY)
        inside = pl.BlockSpec(memory_space=pltpu.VMEM)
        vectors = (mix_gain, ffn_gain, in_scale, out_scale, gate_scale, up_scale, down_scale)
        return pl.pallas_call(
            fused,
            out_shape=jax.ShapeDtypeStruct((rows, cols), low_type),
            in_specs=[anywhere] * 6 + [inside] * len(vectors),
            out_specs=anywhere,
            scratch_shapes=[pltpu.VMEM(shape, kind) for shape, kind in buffers]
            + [pltpu.SemaphoreType.DMA(shape) for shape in semaphores],
            compiler_params=pltpu.CompilerParams(
                collective_id=0, has_side_effects=True, vmem_limit_bytes=67043328
            ),
        )(
            tokens,
            in_weight,
            out_weight,
            gate_weight,
            up_weight,
            down_weight,
            *vectors,
        )

    return jax.shard_map(
        local, mesh=mesh, in_specs=IN_SPECS, out_specs=P("fs", "tp"), check_vma=False
    )


def solution(mesh):
    fs, tp = mesh.shape["fs"], mesh.shape["tp"]
    xs = max(tp // 2, 1)
    return paired(mesh) if (xs, fs // xs) == (2, 4) else general(mesh)
```

```python
import jax
import jax.numpy as jnp
from jax import lax
from jax.experimental import pallas as pl
from jax.experimental.pallas import tpu as pltpu
from jax.sharding import PartitionSpec as P

GROUPS = 4
GRID_W = 64
GC = 256
WINDOWS = (2, 4, 8, 16)
EPSILON = 1e-06


IN_SPECS = (
    P("fs", "tp"),
    P(),
    P("fs", "tp"),
    P("tp"),
    P("tp", "fs"),
    P("fs"),
    P(),
    P("fs", "tp"),
    P("tp"),
    P("fs", "tp"),
    P("tp"),
    P("tp", "fs"),
    P("fs"),
)


def box_matrix(length, window):
    position = jnp.arange(length, dtype=jnp.int32)
    lower_end = jnp.clip(position - window // 2, 0, length)
    upper_end = jnp.clip(position + (window - window // 2), 0, length)
    inside = (position[None, :] >= lower_end[:, None]) & (position[None, :] < upper_end[:, None])
    return inside.astype(jnp.float32) / (upper_end - lower_end).astype(jnp.float32)[:, None]


def smooth(lattice, window):
    across = jnp.einsum(
        "jk,akc->ajc", box_matrix(GRID_W, window), lattice, precision=lax.Precision.HIGHEST
    )
    return jnp.einsum(
        "ab,bjc->ajc",
        box_matrix(lattice.shape[0], window),
        across,
        precision=lax.Precision.HIGHEST,
    )


def pooled_differences(channels, channel_offset):
    tokens_here, extent = channels.shape
    lattice = channels.reshape(tokens_here // GRID_W, GRID_W, extent)
    if GC % extent == 0:
        result = smooth(lattice, jnp.asarray(WINDOWS, jnp.int32)[channel_offset // GC])
    else:
        group_of = (channel_offset + jnp.arange(extent, dtype=jnp.int32)) // GC
        result = jnp.zeros_like(lattice)
        for group in range(GROUPS):
            result = jnp.where(
                (group_of == group)[None, None, :], smooth(lattice, WINDOWS[group]), result
            )
    return (result - lattice).reshape(tokens_here, extent).astype(jnp.bfloat16)


class Grid:
    def __init__(self, fs, tp):
        self.ys = max(tp // 2, 1)
        self.zs = fs // self.ys
        index = lax.axis_index("fs")
        self.z, self.y = index // self.ys, index % self.ys

    def gather(self, block):
        rows = []
        for s in range(self.zs):
            pairs = [
                (z * self.ys + y, (z + s) % self.zs * self.ys + y)
                for z in range(self.zs)
                for y in range(self.ys)
            ]
            rows.append(lax.ppermute(block, "fs", pairs) if s else block)
        found = []
        for s, row in enumerate(rows):
            for t in range(self.ys):
                pairs = [
                    (z * self.ys + y, z * self.ys + (y + t) % self.ys)
                    for z in range(self.zs)
                    for y in range(self.ys)
                ]
                item = lax.ppermute(row, "fs", pairs) if t else row
                index = lax.rem(self.z - s + self.zs, self.zs) * self.ys + lax.rem(
                    self.y - t + self.ys, self.ys
                )
                found.append((index, item))
        return found


def stack(pieces):
    shape = (len(pieces),) + pieces[0][1].shape
    result = jnp.zeros(shape, pieces[0][1].dtype)
    for index, item in pieces:
        result = lax.dynamic_update_index_in_dim(result, item, index, 0)
    return result


def rows_of(pieces):
    whole = stack(pieces)
    return whole.reshape(whole.shape[0] * whole.shape[1], whole.shape[2])


def fold_rows(features, gain, weights):
    widened = lax.all_gather(features, "tp", axis=1, tiled=True)
    widened = widened.astype(jnp.float32)
    inverse_rms = lax.rsqrt(jnp.mean(widened * widened, axis=1) + EPSILON)[:, None]
    scaled = (widened * gain).astype(jnp.bfloat16)
    return tuple(
        jnp.dot(scaled, weight, preferred_element_type=jnp.float32) * inverse_rms
        for weight in weights
    )


def column_product(hidden, pieces):
    terms = stack(
        [
            (index, jnp.dot(hidden, item, preferred_element_type=jnp.float32).astype(jnp.bfloat16))
            for index, item in pieces
        ]
    )
    mine = lax.psum_scatter(terms, "tp", scatter_dimension=0, tiled=True)
    return mine.transpose(1, 0, 2).reshape(hidden.shape[0], -1).astype(jnp.float32)


def low(weight, scale=None):
    weight = weight.astype(jnp.bfloat16)
    if scale is None:
        return weight
    return (weight.astype(jnp.float32) * scale).astype(jnp.bfloat16)


def general(mesh):
    fs, tp = mesh.shape["fs"], mesh.shape["tp"]

    def layer(
        tokens,
        mix_gain,
        in_weight,
        in_scale,
        out_weight,
        out_scale,
        ffn_gain,
        gate_weight,
        gate_scale,
        up_weight,
        up_scale,
        down_weight,
        down_scale,
    ):
        grid = Grid(fs, tp)
        wide = gate_weight.shape[1]
        both_pieces = grid.gather(jnp.concatenate([low(gate_weight), low(up_weight)], axis=1))
        down_pieces = grid.gather(low(down_weight, down_scale))
        small = lax.all_gather(
            jnp.stack([low(in_weight), low(out_weight, out_scale)]), "fs", axis=0
        )
        in_full = small[:, 0].reshape(-1, in_weight.shape[1])
        out_pieces = [(j, small[j, 1]) for j in range(fs)]
        (channels,) = fold_rows(tokens, mix_gain, (in_full,))
        channels = channels * in_scale
        pooled = pooled_differences(channels, lax.axis_index("tp") * channels.shape[1])
        mixed = column_product(pooled, out_pieces)
        residual = (tokens.astype(jnp.float32) + mixed).astype(jnp.bfloat16)
        (both,) = fold_rows(residual, ffn_gain, (rows_of(both_pieces),))
        gate_value = both[:, :wide] * gate_scale
        up_value = both[:, wide:] * up_scale
        hidden = (jax.nn.silu(gate_value) * up_value).astype(jnp.bfloat16)
        channel_out = column_product(hidden, down_pieces)
        return (residual.astype(jnp.float32) + channel_out).astype(jnp.bfloat16)

    return jax.shard_map(
        layer, mesh=mesh, in_specs=IN_SPECS, out_specs=P("fs", "tp"), check_vma=False
    )


class Place:
    def __init__(self):
        index, column = lax.axis_index("fs"), lax.axis_index("tp")
        z, self.y = index // 2, index % 2
        self.zh, self.zl = z // 2, z % 2
        self.x, self.c = column // 2, column % 2
        self.index, self.column = index, column
        self.to_x = {"tp": (1 - self.x) * 2 + self.c}
        self.to_c = {"tp": self.x * 2 + 1 - self.c}
        self.to_y = {"fs": z * 2 + 1 - self.y}
        self.to_zl = {"fs": (self.zh * 2 + 1 - self.zl) * 2 + self.y}
        self.to_zh = {"fs": ((1 - self.zh) * 2 + self.zl) * 2 + self.y}

    def slot(self, dh, dl, dy):
        zh, zl, y = (self.zh + dh) % 2, (self.zl + dl) % 2, (self.y + dy) % 2
        return (zh * 2 + zl) * 2 + y


class Mail:
    def __init__(self):
        self.started = []

    def make(self, source, target, send_sem, recv_sem, device):
        return pltpu.make_async_remote_copy(
            src_ref=source,
            dst_ref=target,
            send_sem=send_sem,
            recv_sem=recv_sem,
            device_id=device,
            device_id_type=pl.DeviceIdType.MESH,
        )

    def send(self, source, target, send_sem, recv_sem, device):
        copy = self.make(source, target, send_sem, recv_sem, device)
        copy.start()
        self.started.append(copy)
        return copy

    def arrived(self, target, recv_sem):
        pltpu.make_async_copy(target, target, recv_sem).wait()

    def settle(self, copies):
        for copy in copies:
            copy.wait_send()
        self.started = [copy for copy in self.started if all(copy is not c for c in copies)]

    def close(self):
        self.settle(self.started)


class Gather:
    def __init__(self, mail, place, kind, target, sends, recvs):
        self.mail, self.place, self.kind = mail, place, kind
        self.target, self.sends, self.recvs = target, sends, recvs
        self.count = 0

    def pass_on(self, source, slot, device):
        self.mail.send(
            source,
            self.target(slot),
            self.sends.at[self.kind, self.count],
            self.recvs.at[self.kind, slot],
            device,
        )
        self.count += 1

    def forward(self, slot, *devices):
        self.mail.arrived(self.target(slot), self.recvs.at[self.kind, slot])
        for device in devices:
            self.pass_on(self.target(slot), slot, device)

    def rows_y(self, lows=(0, 1)):
        for dl in lows:
            for dh in (0, 1):
                self.forward(self.place.slot(dh, dl, 1))


class WholeGather(Gather):
    def start(self, own):
        p = self.place
        self.pass_on(own, p.index, p.to_zh)
        self.pass_on(own, p.index, p.to_zl)
        self.pass_on(own, p.index, p.to_y)

    def on_zh(self):
        p = self.place
        self.forward(p.slot(1, 0, 0), p.to_zl, p.to_y)

    def on_zl(self):
        p = self.place
        self.forward(p.slot(0, 1, 0), p.to_y)
        self.forward(p.slot(1, 1, 0), p.to_y)


class HalfGather(Gather):
    def start_zl(self, other):
        self.pass_on(other, self.place.index, self.place.to_zl)

    def start_zh(self, own):
        self.pass_on(own, self.place.index, self.place.to_zh)

    def start_y(self, own):
        self.pass_on(own, self.place.index, self.place.to_y)

    def on_zl(self):
        p = self.place
        self.forward(p.slot(0, 1, 0), p.to_zh, p.to_y)

    def on_zh(self, dl):
        p = self.place
        self.forward(p.slot(1, dl, 0), p.to_y)


def lanes(start, size):
    return pl.ds(pl.multiple_of(start, 128), size)


def fused(
    tok, w_in, w_out, w_gate, w_up, w_down,
    gain_mix, gain_ffn, s_in, s_out, s_gate, s_up, s_down, out,
    tokens, res, in_all, out_all, gu_all, dn_all, hid, mask, chan, high, low_part, pooled,
    mix_cs, mix_cr, mix_own, mix_xs, mix_xr,
    sum_cs, sum_cr, sum_xs, sum_xr, sum_zs, sum_zr, done,
    f_in, f_out, f_gate, f_up, f_down, gu_other, dn_other,
    local_sem, w_send, w_recv, t_send, t_recv, r_send, r_recv, m_send, m_recv,
    c_send, c_recv, x_send, x_recv, z_send, z_recv,
):
    rows, features = tokens.shape
    cols = tok.shape[1]
    block = w_in.shape[0]
    unit_hidden = dn_all.shape[1]
    half = gu_all.shape[2] // 2
    chunk = rows // 4
    tall = rows // 2
    p, mail = Place(), Mail()

    def kept(kind):
        return {
            0: lambda j: in_all.at[pl.ds(pl.multiple_of(j * block, 16), block), :],
            1: lambda j: out_all.at[j],
            2: lambda j: gu_all.at[0, pl.ds(pl.multiple_of(j * block, 16), block), :],
            3: lambda j: gu_all.at[1, pl.ds(pl.multiple_of(j * block, 16), block), :],
            4: lambda j: dn_all.at[j],
        }[kind]

    g_in, g_out = (WholeGather(mail, p, k, kept(k), w_send, w_recv) for k in (0, 1))
    g_gu = [HalfGather(mail, p, 2 + q, kept(2 + q), w_send, w_recv) for q in (0, 1)]
    g_dn = HalfGather(mail, p, 4, kept(4), w_send, w_recv)

    def piece(k):
        return pl.ds(k * chunk, chunk)

    def column_of(dx, dc):
        return ((p.x + dx) % 2) * 2 + (p.c + dc) % 2

    copies = [
        pltpu.make_async_copy(source, target, local_sem.at[n])
        for n, (source, target) in enumerate((
            (w_in, f_in),
            (w_out, f_out),
            (tok, tokens.at[:, lanes(p.column * cols, cols)]),
            (w_gate, f_gate),
            (w_up, f_up),
            (w_down, f_down),
        ))
    ]
    for copy in copies:
        copy.start()
    barrier = pltpu.get_barrier_semaphore()
    for device in (p.to_c, p.to_x, p.to_y, p.to_zl, p.to_zh):
        pl.semaphore_signal(
            barrier, inc=1, device_id=device, device_id_type=pl.DeviceIdType.MESH
        )
    pl.semaphore_wait(barrier, 5)
    for k in range(4):
        own = tok.at[piece(k), :]
        at = tokens.at[piece(k), lanes(p.column * cols, cols)]
        mail.send(own, at, t_send.at[0, k], t_recv.at[p.column, k], p.to_x)
        mail.send(own, at, t_send.at[1, k], t_recv.at[p.column, k], p.to_c)

    def rounded(weight, scale):
        weight = weight.astype(jnp.bfloat16).astype(jnp.float32)
        return (weight * scale[None, :]).astype(jnp.bfloat16)

    copies[0].wait()
    kept(0)(p.index)[...] = rounded(f_in[...], s_in[...])
    g_in.start(kept(0)(p.index))
    copies[1].wait()
    kept(1)(p.index)[...] = rounded(f_out[...], s_out[...])
    g_out.start(kept(1)(p.index))
    for copy in copies[3:]:
        copy.wait()
    for q in (0, 1):
        for own in (True, False):
            target = kept(2 + q)(p.index) if own else gu_other.at[q]
            at = lanes(((p.zl if own else 1 - p.zl) * 2 + q) * half, half)
            target[:, :half] = rounded(f_gate[:, at], s_gate[at])
            target[:, half:] = rounded(f_up[:, at], s_up[at])
    for own in (True, False):
        target = kept(4)(p.index) if own else dn_other
        at = (p.zl if own else 1 - p.zl) * unit_hidden
        at = pl.ds(pl.multiple_of(at, 16), unit_hidden)
        target[...] = rounded(f_down[at, :], s_down[...])

    window = lax.shift_left(2, p.column * block // GC)
    below = window // 2
    above = window - below

    def mask_rows(i, _):
        cell = i * chunk // 2 + lax.broadcasted_iota(jnp.int32, (chunk // 2, rows), 0)
        other = lax.broadcasted_iota(jnp.int32, (chunk // 2, rows), 1)
        dr = other // GRID_W - cell // GRID_W
        dc = other % GRID_W - cell % GRID_W
        inside = (dr >= -below) & (dr < above) & (dc >= -below) & (dc < above)
        at = pl.ds(pl.multiple_of(i * (chunk // 2), 16), chunk // 2)
        mask[at, :] = jnp.where(inside, 1.0, 0.0).astype(jnp.bfloat16)
        return 0

    lax.fori_loop(0, 8, mask_rows, 0)

    g_in.on_zh()
    g_out.on_zh()
    g_in.on_zl()
    g_out.on_zl()
    for q in (0, 1):
        g_gu[q].start_zl(gu_other.at[q])
    for q in (0, 1):
        g_gu[q].start_zh(kept(2 + q)(p.index))
    for q in (0, 1):
        g_gu[q].start_y(kept(2 + q)(p.index))
    g_dn.start_y(kept(4)(p.index))

    def token_at(column, k):
        return tokens.at[piece(k), lanes(column * cols, cols)]

    passed = []
    for k in range(4):
        column = column_of(1, 0)
        here = token_at(column, k)
        mail.arrived(here, t_recv.at[column, k])
        passed.append(mail.send(here, here, t_send.at[2, k], t_recv.at[column, k], p.to_c))
    copies[2].wait()
    for dx in (0, 1):
        for k in range(4):
            column = column_of(dx, 1)
            mail.arrived(token_at(column, k), t_recv.at[column, k])
    g_in.rows_y()

    def normed(wide, gain):
        square = wide * wide
        scale = lax.rsqrt(jnp.sum(square, axis=1, keepdims=True) / features + EPSILON)
        return (wide * gain[...][None, :]).astype(jnp.bfloat16), scale

    def channel_rows(i, _):
        at = pl.ds(pl.multiple_of(i * chunk, 16), chunk)
        wide, scale = normed(tokens[at, :].astype(jnp.float32), gain_mix)
        value = jnp.dot(wide, in_all[...], preferred_element_type=jnp.float32) * scale
        chan[at, :] = value
        first = value.astype(jnp.bfloat16)
        high[at, :] = first
        low_part[at, :] = (value - first.astype(jnp.float32)).astype(jnp.bfloat16)
        return 0

    lax.fori_loop(0, 4, channel_rows, 0)

    def extent(position, length):
        upper = jnp.minimum(position + above, length)
        return upper - jnp.maximum(position - below, 0)

    def pool_rows(i, _):
        at = pl.ds(pl.multiple_of(i * chunk, 16), chunk)
        inside = mask[at, :]
        total = jnp.dot(inside, high[...], preferred_element_type=jnp.float32) + jnp.dot(
            inside, low_part[...], preferred_element_type=jnp.float32
        )
        cell = i * chunk + lax.broadcasted_iota(jnp.int32, (chunk, block), 0)
        cells = extent(cell // GRID_W, rows // GRID_W) * extent(cell % GRID_W, GRID_W)
        pooled[at, :] = (total / cells.astype(jnp.float32) - chan[at, :]).astype(jnp.bfloat16)
        return 0

    lax.fori_loop(0, 4, pool_rows, 0)

    g_out.rows_y()

    for k in range(4):
        part = pooled[piece(k), :]
        for dx in (0, 1):
            for dc in (0, 1):
                target = mix_own if dc == 0 else mix_cs
                for side in (0, 1):
                    j = column_of(dx, dc) * 2 + side
                    term = jnp.dot(part, out_all[j], preferred_element_type=jnp.float32)
                    target[k, dx, :, side * block:(side + 1) * block] = term.astype(jnp.bfloat16)
        mail.send(mix_cs.at[k], mix_cr.at[k], m_send.at[0, k], m_recv.at[0, k], p.to_c)

    def both(k, dx):
        return mix_own[k, dx].astype(jnp.float32) + mix_cr[k, dx].astype(jnp.float32)

    for k in range(4):
        mail.arrived(mix_cr.at[k], m_recv.at[0, k])
        mix_xs[k] = both(k, 1).astype(jnp.bfloat16)
        mail.send(mix_xs.at[k], mix_xr.at[k], m_send.at[1, k], m_recv.at[1, k], p.to_x)

    def res_at(dz, column, k):
        return res.at[(p.zl + dz) % 2, piece(k), lanes(column * cols, cols)]

    def res_send(dz, column, k, lane, device):
        here = res_at(dz, column, k)
        sem = ((p.zl + dz) % 2) * 4 + column
        mail.send(here, here, r_send.at[lane, k], r_recv.at[sem, k], device)

    def res_wait(dz, column, k):
        sem = ((p.zl + dz) % 2) * 4 + column
        mail.arrived(res_at(dz, column, k), r_recv.at[sem, k])

    for k in range(4):
        mail.arrived(mix_xr.at[k], m_recv.at[1, k])
        mine = lanes(p.column * cols, cols)
        total = both(k, 0) + mix_xr[k].astype(jnp.float32)
        total = total + tokens[piece(k), mine].astype(jnp.float32)
        res[p.zl, piece(k), mine] = total.astype(jnp.bfloat16)
        res_send(0, p.column, k, 0, p.to_x)
        res_send(0, p.column, k, 1, p.to_zl)
        res_send(0, p.column, k, 2, p.to_c)
        if k > 1:
            g_gu[k - 2].on_zl()
    g_dn.start_zl(dn_other)

    across = column_of(1, 0)

    def on_x(k):
        res_wait(0, across, k)
        res_send(0, across, k, 5, p.to_c)

    def on_z(k):
        res_wait(1, p.column, k)
        res_send(1, p.column, k, 3, p.to_x)
        res_send(1, p.column, k, 4, p.to_c)

    def on_both(k):
        res_wait(1, across, k)
        res_send(1, across, k, 6, p.to_c)

    on_x(0)
    g_gu[0].on_zh(0)
    on_x(1)
    g_gu[1].on_zh(0)
    on_x(2)
    on_z(0)
    on_x(3)
    on_z(1)
    g_gu[0].on_zh(1)
    g_dn.start_zh(kept(4)(p.index))
    g_gu[1].on_zh(1)
    on_z(2)
    on_both(0)
    on_both(1)
    for k in range(4):
        for dx in (0, 1):
            res_wait(0, column_of(dx, 1), k)
    g_gu[0].rows_y()

    def hidden_rows(dz, *halves):
        def body(i, _):
            at = pl.ds(pl.multiple_of(i * chunk, 16), chunk)
            z = (p.zl + dz) % 2
            wide, scale = normed(res[z, at, :].astype(jnp.float32), gain_ffn)
            for q in halves:
                value = jnp.dot(wide, gu_all[q], preferred_element_type=jnp.float32) * scale
                gate, up = value[:, :half], value[:, half:]
                unit = gate / (1.0 + jnp.exp(-gate)) * up
                hid[z, at, q * half:(q + 1) * half] = unit.astype(jnp.bfloat16)
            return 0

        return body

    lax.fori_loop(0, 4, hidden_rows(0, 0), 0)
    on_z(3)
    g_gu[1].rows_y()
    lax.fori_loop(0, 2, hidden_rows(0, 1), 0)
    g_dn.on_zl()
    lax.fori_loop(2, 4, hidden_rows(0, 1), 0)
    on_both(2)
    on_both(3)
    g_dn.on_zh(0)
    for k in range(4):
        for dx in (0, 1):
            res_wait(1, column_of(dx, 1), k)
    lax.fori_loop(0, 4, hidden_rows(1, 0, 1), 0)

    mail.settle(passed)

    def mine(group):
        return (p.c + p.zl + group) % 2 == 0

    def unit(dy, dz, k):
        return dy * 4 + dz * 2 + k

    def sum_own(u, dx):
        return tokens.at[pl.ds((u % 2) * tall, tall), pl.ds((u // 2 * 2 + dx) * block, block)]

    def pair(u, dx):
        return sum_own(u, dx)[...].astype(jnp.float32) + sum_cr[u, dx].astype(jnp.float32)

    def out_part(dy, k):
        return pl.ds(k * tall, tall), lanes((p.y + dy) % 2 * block, block)

    c_copies = [
        mail.make(sum_cs.at[u], sum_cr.at[u], c_send.at[u], c_recv.at[u], p.to_c) for u in range(8)
    ]
    x_copies = [
        mail.make(sum_xs.at[n], sum_xr.at[n], x_send.at[n], x_recv.at[n], p.to_x) for n in range(6)
    ]
    z_copies = [
        mail.make(sum_zs.at[n], sum_zr.at[n], z_send.at[n], z_recv.at[n], p.to_zl) for n in range(6)
    ]
    mail.started += c_copies + x_copies + z_copies
    results = [
        pltpu.make_async_copy(
            done.at[out_part(n // 2, n % 2)], out.at[out_part(n // 2, n % 2)], local_sem.at[n]
        )
        for n in range(4)
    ]

    def stage_core(group, dy, dz, k):
        u = unit(dy, dz, k)

        def term(dx):
            j = (((p.x + dx) % 2) * 2 + (p.zl + group) % 2) * 2 + (p.y + dy) % 2
            part = hid[(p.zl + dz) % 2, pl.ds(k * tall, tall), :]
            value = jnp.dot(part, dn_all[j], preferred_element_type=jnp.float32)
            return value.astype(jnp.bfloat16)

        @pl.when(mine(group))
        def _():
            for dx in (0, 1):
                sum_own(u, dx)[...] = term(dx)

        @pl.when(mine(1 - group))
        def _():
            for dx in (0, 1):
                sum_cs[u, dx] = term(dx)
            c_copies[u].start()

    def stage_first(group, dy, dz, k):
        u = unit(dy, dz, k)

        @pl.when(mine(group))
        def _():
            mail.arrived(sum_cr.at[u], c_recv.at[u])
            if k == 0:
                n = dy * 3 + dz
                sum_xs[n] = pair(u, 1).astype(jnp.bfloat16)
                x_copies[n].start()
            elif dz == 1:
                for dx in (1, 0):
                    n = dy * 3 + dx
                    sum_zs[n] = pair(u, dx).astype(jnp.bfloat16)
                    z_copies[n].start()

    def from_x(group, dy):
        n = dy * 3

        @pl.when(mine(group))
        def _():
            mail.arrived(sum_xr.at[n + 1], x_recv.at[n + 1])
            total = pair(unit(dy, 1, 0), 0) + sum_xr[n + 1].astype(jnp.float32)
            sum_zs[n + 2] = total.astype(jnp.bfloat16)
            z_copies[n + 2].start()

    def from_z(group, dy):
        n = dy * 3

        @pl.when(mine(group))
        def _():
            mail.arrived(sum_zr.at[n + 1], z_recv.at[n + 1])
            total = pair(unit(dy, 0, 1), 1) + sum_zr[n + 1].astype(jnp.float32)
            sum_xs[n + 2] = total.astype(jnp.bfloat16)
            x_copies[n + 2].start()

    def stage_last(dy, k):
        n = dy * 3
        first, second = (n, n + 2) if k == 0 else (n + 2, n)
        mail.arrived(sum_xr.at[first], x_recv.at[first])
        mail.arrived(sum_zr.at[second], z_recv.at[second])
        total = pair(unit(dy, 0, k), 0)
        total = total + sum_xr[first].astype(jnp.float32) + sum_zr[second].astype(jnp.float32)
        at = pl.ds(k * tall, tall)
        side = p.column * cols + (p.y + dy) % 2 * block
        total = total + res[p.zl, at, lanes(side, block)].astype(jnp.float32)
        done[out_part(dy, k)] = total.astype(jnp.bfloat16)
        results[dy * 2 + k].start()

    order = [(1, 0), (0, 0), (1, 1), (0, 1)]

    def stage_all(group, dy):
        for n, (dz, k) in enumerate(order):
            stage_core(group, dy, dz, k)
            if n > 1:
                stage_first(group, dy, *order[n - 2])
        for n in (2, 3):
            stage_first(group, dy, *order[n])

    stage_all(0, 0)
    g_dn.on_zh(1)
    g_dn.rows_y((0,))
    stage_all(0, 1)
    stage_all(1, 0)
    from_x(0, 0)
    g_dn.rows_y((1,))
    stage_all(1, 1)
    from_z(0, 0)
    from_x(0, 1)
    from_z(0, 1)
    for dy in (0, 1):
        from_x(1, dy)
        from_z(1, dy)
    for dy in (0, 1):
        for k in (0, 1):
            stage_last(dy, k)
    mail.close()
    for copy in results:
        copy.wait()


def paired(mesh):
    fs, tp = mesh.shape["fs"], mesh.shape["tp"]

    def local(
        tokens,
        mix_gain,
        in_weight,
        in_scale,
        out_weight,
        out_scale,
        ffn_gain,
        gate_weight,
        gate_scale,
        up_weight,
        up_scale,
        down_weight,
        down_scale,
    ):
        rows, cols = tokens.shape
        depth, block = in_weight.shape
        wide = gate_weight.shape[1]
        features = cols * tp
        low_type = jnp.bfloat16
        tall = rows // 2
        buffers = [
            ((rows, features), low_type),
            ((2, rows, features), low_type),
            ((features, block), low_type),
            ((fs, block, block), low_type),
            ((2, features, wide // 2), low_type),
            ((fs, wide // 2, block), low_type),
            ((2, rows, wide // 2), low_type),
            ((rows, rows), low_type),
            ((rows, block), jnp.float32),
            ((rows, block), low_type),
            ((rows, block), low_type),
            ((rows, block), low_type),
            ((4, 2, rows // 4, cols), low_type),
            ((4, 2, rows // 4, cols), low_type),
            ((4, 2, rows // 4, cols), low_type),
            ((4, rows // 4, cols), low_type),
            ((4, rows // 4, cols), low_type),
            ((8, 2, tall, block), low_type),
            ((8, 2, tall, block), low_type),
            ((6, tall, block), low_type),
            ((6, tall, block), low_type),
            ((6, tall, block), low_type),
            ((6, tall, block), low_type),
            ((rows, cols), low_type),
            (in_weight.shape, jnp.float32),
            (out_weight.shape, jnp.float32),
            (gate_weight.shape, jnp.float32),
            (up_weight.shape, jnp.float32),
            (down_weight.shape, jnp.float32),
            ((2, depth, wide // 2), low_type),
            ((wide // 2, block), low_type),
        ]
        semaphores = [(6,), (5, 7), (5, fs), (3, 4), (tp, 4), (7, 4), (2 * tp, 4), (2, 4), (2, 4)]
        semaphores += [(8,), (8,), (6,), (6,), (6,), (6,)]
        anywhere = pl.BlockSpec(memory_space=pl.ANY)
        inside = pl.BlockSpec(memory_space=pltpu.VMEM)
        vectors = (mix_gain, ffn_gain, in_scale, out_scale, gate_scale, up_scale, down_scale)
        return pl.pallas_call(
            fused,
            out_shape=jax.ShapeDtypeStruct((rows, cols), low_type),
            in_specs=[anywhere] * 6 + [inside] * len(vectors),
            out_specs=anywhere,
            scratch_shapes=[pltpu.VMEM(shape, kind) for shape, kind in buffers]
            + [pltpu.SemaphoreType.DMA(shape) for shape in semaphores],
            compiler_params=pltpu.CompilerParams(
                collective_id=0, has_side_effects=True, vmem_limit_bytes=67043328
            ),
        )(
            tokens,
            in_weight,
            out_weight,
            gate_weight,
            up_weight,
            down_weight,
            *vectors,
        )

    return jax.shard_map(
        local, mesh=mesh, in_specs=IN_SPECS, out_specs=P("fs", "tp"), check_vma=False
    )


def solution(mesh):
    fs, tp = mesh.shape["fs"], mesh.shape["tp"]
    xs = max(tp // 2, 1)
    return paired(mesh) if (xs, fs // xs) == (2, 4) else general(mesh)
```

```python
import jax
import jax.numpy as jnp
from jax import lax
from jax.experimental import pallas as pl
from jax.experimental.pallas import tpu as pltpu
from jax.sharding import PartitionSpec as P

GROUPS = 4
GRID_W = 64
GC = 256
WINDOWS = (2, 4, 8, 16)
EPSILON = 1e-06


IN_SPECS = (
    P("fs", "tp"),
    P(),
    P("fs", "tp"),
    P("tp"),
    P("tp", "fs"),
    P("fs"),
    P(),
    P("fs", "tp"),
    P("tp"),
    P("fs", "tp"),
    P("tp"),
    P("tp", "fs"),
    P("fs"),
)


def box_matrix(length, window):
    position = jnp.arange(length, dtype=jnp.int32)
    lower_end = jnp.clip(position - window // 2, 0, length)
    upper_end = jnp.clip(position + (window - window // 2), 0, length)
    inside = (position[None, :] >= lower_end[:, None]) & (position[None, :] < upper_end[:, None])
    return inside.astype(jnp.float32) / (upper_end - lower_end).astype(jnp.float32)[:, None]


def smooth(lattice, window):
    across = jnp.einsum(
        "jk,akc->ajc", box_matrix(GRID_W, window), lattice, precision=lax.Precision.HIGHEST
    )
    return jnp.einsum(
        "ab,bjc->ajc",
        box_matrix(lattice.shape[0], window),
        across,
        precision=lax.Precision.HIGHEST,
    )


def pooled_differences(channels, channel_offset):
    tokens_here, extent = channels.shape
    lattice = channels.reshape(tokens_here // GRID_W, GRID_W, extent)
    if GC % extent == 0:
        result = smooth(lattice, jnp.asarray(WINDOWS, jnp.int32)[channel_offset // GC])
    else:
        group_of = (channel_offset + jnp.arange(extent, dtype=jnp.int32)) // GC
        result = jnp.zeros_like(lattice)
        for group in range(GROUPS):
            result = jnp.where(
                (group_of == group)[None, None, :], smooth(lattice, WINDOWS[group]), result
            )
    return (result - lattice).reshape(tokens_here, extent).astype(jnp.bfloat16)


class Grid:
    def __init__(self, fs, tp):
        self.ys = max(tp // 2, 1)
        self.zs = fs // self.ys
        index = lax.axis_index("fs")
        self.z, self.y = index // self.ys, index % self.ys

    def gather(self, block):
        rows = []
        for s in range(self.zs):
            pairs = [
                (z * self.ys + y, (z + s) % self.zs * self.ys + y)
                for z in range(self.zs)
                for y in range(self.ys)
            ]
            rows.append(lax.ppermute(block, "fs", pairs) if s else block)
        found = []
        for s, row in enumerate(rows):
            for t in range(self.ys):
                pairs = [
                    (z * self.ys + y, z * self.ys + (y + t) % self.ys)
                    for z in range(self.zs)
                    for y in range(self.ys)
                ]
                item = lax.ppermute(row, "fs", pairs) if t else row
                index = lax.rem(self.z - s + self.zs, self.zs) * self.ys + lax.rem(
                    self.y - t + self.ys, self.ys
                )
                found.append((index, item))
        return found


def stack(pieces):
    shape = (len(pieces),) + pieces[0][1].shape
    result = jnp.zeros(shape, pieces[0][1].dtype)
    for index, item in pieces:
        result = lax.dynamic_update_index_in_dim(result, item, index, 0)
    return result


def rows_of(pieces):
    whole = stack(pieces)
    return whole.reshape(whole.shape[0] * whole.shape[1], whole.shape[2])


def fold_rows(features, gain, weights):
    widened = lax.all_gather(features, "tp", axis=1, tiled=True)
    widened = widened.astype(jnp.float32)
    inverse_rms = lax.rsqrt(jnp.mean(widened * widened, axis=1) + EPSILON)[:, None]
    scaled = (widened * gain).astype(jnp.bfloat16)
    return tuple(
        jnp.dot(scaled, weight, preferred_element_type=jnp.float32) * inverse_rms
        for weight in weights
    )


def column_product(hidden, pieces):
    terms = stack(
        [
            (index, jnp.dot(hidden, item, preferred_element_type=jnp.float32).astype(jnp.bfloat16))
            for index, item in pieces
        ]
    )
    mine = lax.psum_scatter(terms, "tp", scatter_dimension=0, tiled=True)
    return mine.transpose(1, 0, 2).reshape(hidden.shape[0], -1).astype(jnp.float32)


def low(weight, scale=None):
    weight = weight.astype(jnp.bfloat16)
    if scale is None:
        return weight
    return (weight.astype(jnp.float32) * scale).astype(jnp.bfloat16)


def general(mesh):
    fs, tp = mesh.shape["fs"], mesh.shape["tp"]

    def layer(
        tokens,
        mix_gain,
        in_weight,
        in_scale,
        out_weight,
        out_scale,
        ffn_gain,
        gate_weight,
        gate_scale,
        up_weight,
        up_scale,
        down_weight,
        down_scale,
    ):
        grid = Grid(fs, tp)
        wide = gate_weight.shape[1]
        both_pieces = grid.gather(jnp.concatenate([low(gate_weight), low(up_weight)], axis=1))
        down_pieces = grid.gather(low(down_weight, down_scale))
        small = lax.all_gather(
            jnp.stack([low(in_weight), low(out_weight, out_scale)]), "fs", axis=0
        )
        in_full = small[:, 0].reshape(-1, in_weight.shape[1])
        out_pieces = [(j, small[j, 1]) for j in range(fs)]
        (channels,) = fold_rows(tokens, mix_gain, (in_full,))
        channels = channels * in_scale
        pooled = pooled_differences(channels, lax.axis_index("tp") * channels.shape[1])
        mixed = column_product(pooled, out_pieces)
        residual = (tokens.astype(jnp.float32) + mixed).astype(jnp.bfloat16)
        (both,) = fold_rows(residual, ffn_gain, (rows_of(both_pieces),))
        gate_value = both[:, :wide] * gate_scale
        up_value = both[:, wide:] * up_scale
        hidden = (jax.nn.silu(gate_value) * up_value).astype(jnp.bfloat16)
        channel_out = column_product(hidden, down_pieces)
        return (residual.astype(jnp.float32) + channel_out).astype(jnp.bfloat16)

    return jax.shard_map(
        layer, mesh=mesh, in_specs=IN_SPECS, out_specs=P("fs", "tp"), check_vma=False
    )


class Place:
    def __init__(self):
        index, column = lax.axis_index("fs"), lax.axis_index("tp")
        z, self.y = index // 2, index % 2
        self.zh, self.zl = z // 2, z % 2
        self.x, self.c = column // 2, column % 2
        self.index, self.column = index, column
        self.to_x = {"tp": (1 - self.x) * 2 + self.c}
        self.to_c = {"tp": self.x * 2 + 1 - self.c}
        self.to_y = {"fs": z * 2 + 1 - self.y}
        self.to_zl = {"fs": (self.zh * 2 + 1 - self.zl) * 2 + self.y}
        self.to_zh = {"fs": ((1 - self.zh) * 2 + self.zl) * 2 + self.y}

    def slot(self, dh, dl, dy):
        zh, zl, y = (self.zh + dh) % 2, (self.zl + dl) % 2, (self.y + dy) % 2
        return (zh * 2 + zl) * 2 + y


class Mail:
    def __init__(self):
        self.started = []

    def make(self, source, target, send_sem, recv_sem, device):
        return pltpu.make_async_remote_copy(
            src_ref=source,
            dst_ref=target,
            send_sem=send_sem,
            recv_sem=recv_sem,
            device_id=device,
            device_id_type=pl.DeviceIdType.MESH,
        )

    def send(self, source, target, send_sem, recv_sem, device):
        copy = self.make(source, target, send_sem, recv_sem, device)
        copy.start()
        self.started.append(copy)
        return copy

    def arrived(self, target, recv_sem):
        pltpu.make_async_copy(target, target, recv_sem).wait()

    def settle(self, copies):
        for copy in copies:
            copy.wait_send()
        self.started = [copy for copy in self.started if all(copy is not c for c in copies)]

    def close(self):
        self.settle(self.started)


class Gather:
    def __init__(self, mail, place, kind, target, sends, recvs):
        self.mail, self.place, self.kind = mail, place, kind
        self.target, self.sends, self.recvs = target, sends, recvs
        self.count = 0

    def pass_on(self, source, slot, device):
        self.mail.send(
            source,
            self.target(slot),
            self.sends.at[self.kind, self.count],
            self.recvs.at[self.kind, slot],
            device,
        )
        self.count += 1

    def forward(self, slot, *devices):
        self.mail.arrived(self.target(slot), self.recvs.at[self.kind, slot])
        for device in devices:
            self.pass_on(self.target(slot), slot, device)

    def rows_y(self, lows=(0, 1)):
        for dl in lows:
            for dh in (0, 1):
                self.forward(self.place.slot(dh, dl, 1))


class WholeGather(Gather):
    def start(self, own):
        p = self.place
        self.pass_on(own, p.index, p.to_zh)
        self.pass_on(own, p.index, p.to_zl)
        self.pass_on(own, p.index, p.to_y)

    def on_zh(self):
        p = self.place
        self.forward(p.slot(1, 0, 0), p.to_zl, p.to_y)

    def on_zl(self):
        p = self.place
        self.forward(p.slot(0, 1, 0), p.to_y)
        self.forward(p.slot(1, 1, 0), p.to_y)


class HalfGather(Gather):
    def start_zl(self, other):
        self.pass_on(other, self.place.index, self.place.to_zl)

    def start_zh(self, own):
        self.pass_on(own, self.place.index, self.place.to_zh)

    def start_y(self, own):
        self.pass_on(own, self.place.index, self.place.to_y)

    def on_zl(self):
        p = self.place
        self.forward(p.slot(0, 1, 0), p.to_zh, p.to_y)

    def on_zh(self, dl):
        p = self.place
        self.forward(p.slot(1, dl, 0), p.to_y)


X_FIRST = ((0, 0), (0, 1), (1, 0))


def lanes(start, size):
    return pl.ds(pl.multiple_of(start, 128), size)


def fused(
    tok, w_in, w_out, w_gate, w_up, w_down,
    gain_mix, gain_ffn, s_in, s_out, s_gate, s_up, s_down, out,
    tokens, res, in_all, out_all, gu_all, dn_all, hid, mask, chan, high, low_part, pooled,
    mix_cs, mix_cr, mix_own, mix_xs, mix_xr,
    sum_cs, sum_cr, sum_xs, sum_xr, sum_zr, done,
    f_in, f_out, f_gate, f_up, f_down, gu_other, dn_other,
    local_sem, w_send, w_recv, t_send, t_recv, r_send, r_recv, m_send, m_recv,
    c_send, c_recv, x_send, x_recv, z_send, z_recv,
):
    rows, features = tokens.shape
    cols = tok.shape[1]
    block = w_in.shape[0]
    unit_hidden = dn_all.shape[1]
    half = gu_all.shape[2] // 2
    chunk = rows // 4
    tall = rows // 2
    p, mail = Place(), Mail()

    def kept(kind):
        return {
            0: lambda j: in_all.at[pl.ds(pl.multiple_of(j * block, 16), block), :],
            1: lambda j: out_all.at[j],
            2: lambda j: gu_all.at[0, pl.ds(pl.multiple_of(j * block, 16), block), :],
            3: lambda j: gu_all.at[1, pl.ds(pl.multiple_of(j * block, 16), block), :],
            4: lambda j: dn_all.at[j],
        }[kind]

    g_in, g_out = (WholeGather(mail, p, k, kept(k), w_send, w_recv) for k in (0, 1))
    g_gu = [HalfGather(mail, p, 2 + q, kept(2 + q), w_send, w_recv) for q in (0, 1)]
    g_dn = HalfGather(mail, p, 4, kept(4), w_send, w_recv)

    def piece(k):
        return pl.ds(k * chunk, chunk)

    def column_of(dx, dc):
        return ((p.x + dx) % 2) * 2 + (p.c + dc) % 2

    copies = [
        pltpu.make_async_copy(source, target, local_sem.at[n])
        for n, (source, target) in enumerate((
            (w_in, f_in),
            (w_out, f_out),
            (tok, tokens.at[:, lanes(p.column * cols, cols)]),
            (w_gate, f_gate),
            (w_up, f_up),
            (w_down, f_down),
        ))
    ]
    for copy in copies:
        copy.start()
    barrier = pltpu.get_barrier_semaphore()
    for device in (p.to_c, p.to_x, p.to_y, p.to_zl, p.to_zh):
        pl.semaphore_signal(
            barrier, inc=1, device_id=device, device_id_type=pl.DeviceIdType.MESH
        )
    pl.semaphore_wait(barrier, 5)
    for k in range(4):
        own = tok.at[piece(k), :]
        at = tokens.at[piece(k), lanes(p.column * cols, cols)]
        mail.send(own, at, t_send.at[0, k], t_recv.at[p.column, k], p.to_x)
        mail.send(own, at, t_send.at[1, k], t_recv.at[p.column, k], p.to_c)

    def rounded(weight, scale):
        weight = weight.astype(jnp.bfloat16).astype(jnp.float32)
        return (weight * scale[None, :]).astype(jnp.bfloat16)

    copies[0].wait()
    kept(0)(p.index)[...] = rounded(f_in[...], s_in[...])
    g_in.start(kept(0)(p.index))
    copies[1].wait()
    kept(1)(p.index)[...] = rounded(f_out[...], s_out[...])
    g_out.start(kept(1)(p.index))
    for copy in copies[3:]:
        copy.wait()
    for q in (0, 1):
        for own in (True, False):
            target = kept(2 + q)(p.index) if own else gu_other.at[q]
            at = lanes(((p.zl if own else 1 - p.zl) * 2 + q) * half, half)
            target[:, :half] = rounded(f_gate[:, at], s_gate[at])
            target[:, half:] = rounded(f_up[:, at], s_up[at])
    for own in (True, False):
        target = kept(4)(p.index) if own else dn_other
        at = (p.zl if own else 1 - p.zl) * unit_hidden
        at = pl.ds(pl.multiple_of(at, 16), unit_hidden)
        target[...] = rounded(f_down[at, :], s_down[...])

    window = lax.shift_left(2, p.column * block // GC)
    below = window // 2
    above = window - below

    def mask_rows(i, _):
        cell = i * chunk // 2 + lax.broadcasted_iota(jnp.int32, (chunk // 2, rows), 0)
        other = lax.broadcasted_iota(jnp.int32, (chunk // 2, rows), 1)
        dr = other // GRID_W - cell // GRID_W
        dc = other % GRID_W - cell % GRID_W
        inside = (dr >= -below) & (dr < above) & (dc >= -below) & (dc < above)
        at = pl.ds(pl.multiple_of(i * (chunk // 2), 16), chunk // 2)
        mask[at, :] = jnp.where(inside, 1.0, 0.0).astype(jnp.bfloat16)
        return 0

    lax.fori_loop(0, 8, mask_rows, 0)

    g_in.on_zh()
    g_out.on_zh()
    g_gu[0].start_zl(gu_other.at[0])
    g_in.on_zl()
    g_out.on_zl()
    g_gu[1].start_zl(gu_other.at[1])
    for q in (0, 1):
        g_gu[q].start_zh(kept(2 + q)(p.index))
    for q in (0, 1):
        g_gu[q].start_y(kept(2 + q)(p.index))
    g_dn.start_y(kept(4)(p.index))

    def token_at(column, k):
        return tokens.at[piece(k), lanes(column * cols, cols)]

    passed = []
    for k in range(4):
        column = column_of(1, 0)
        here = token_at(column, k)
        mail.arrived(here, t_recv.at[column, k])
        passed.append(mail.send(here, here, t_send.at[2, k], t_recv.at[column, k], p.to_c))
    copies[2].wait()
    for dx in (0, 1):
        for k in range(4):
            column = column_of(dx, 1)
            mail.arrived(token_at(column, k), t_recv.at[column, k])
    g_in.rows_y()

    def normed(wide, gain):
        square = wide * wide
        scale = lax.rsqrt(jnp.sum(square, axis=1, keepdims=True) / features + EPSILON)
        return (wide * gain[...][None, :]).astype(jnp.bfloat16), scale

    def channel_rows(i, _):
        at = pl.ds(pl.multiple_of(i * chunk, 16), chunk)
        wide, scale = normed(tokens[at, :].astype(jnp.float32), gain_mix)
        value = jnp.dot(wide, in_all[...], preferred_element_type=jnp.float32) * scale
        chan[at, :] = value
        first = value.astype(jnp.bfloat16)
        high[at, :] = first
        low_part[at, :] = (value - first.astype(jnp.float32)).astype(jnp.bfloat16)
        return 0

    lax.fori_loop(0, 4, channel_rows, 0)

    def extent(position, length):
        upper = jnp.minimum(position + above, length)
        return upper - jnp.maximum(position - below, 0)

    def pool_rows(i, _):
        at = pl.ds(pl.multiple_of(i * chunk, 16), chunk)
        inside = mask[at, :]
        total = jnp.dot(inside, high[...], preferred_element_type=jnp.float32) + jnp.dot(
            inside, low_part[...], preferred_element_type=jnp.float32
        )
        cell = i * chunk + lax.broadcasted_iota(jnp.int32, (chunk, block), 0)
        cells = extent(cell // GRID_W, rows // GRID_W) * extent(cell % GRID_W, GRID_W)
        pooled[at, :] = (total / cells.astype(jnp.float32) - chan[at, :]).astype(jnp.bfloat16)
        return 0

    lax.fori_loop(0, 4, pool_rows, 0)

    g_out.rows_y()

    for k in range(4):
        part = pooled[piece(k), :]
        for dx in (0, 1):
            for dc in (0, 1):
                target = mix_own if dc == 0 else mix_cs
                for side in (0, 1):
                    j = column_of(dx, dc) * 2 + side
                    term = jnp.dot(part, out_all[j], preferred_element_type=jnp.float32)
                    target[k, dx, :, side * block:(side + 1) * block] = term.astype(jnp.bfloat16)
        mail.send(mix_cs.at[k], mix_cr.at[k], m_send.at[0, k], m_recv.at[0, k], p.to_c)

    def both(k, dx):
        return mix_own[k, dx].astype(jnp.float32) + mix_cr[k, dx].astype(jnp.float32)

    for k in range(4):
        mail.arrived(mix_cr.at[k], m_recv.at[0, k])
        mix_xs[k] = both(k, 1).astype(jnp.bfloat16)
        mail.send(mix_xs.at[k], mix_xr.at[k], m_send.at[1, k], m_recv.at[1, k], p.to_x)

    def res_at(dz, column, k):
        return res.at[(p.zl + dz) % 2, piece(k), lanes(column * cols, cols)]

    def res_send(dz, column, k, lane, device):
        here = res_at(dz, column, k)
        sem = ((p.zl + dz) % 2) * 4 + column
        mail.send(here, here, r_send.at[lane, k], r_recv.at[sem, k], device)

    def res_wait(dz, column, k):
        sem = ((p.zl + dz) % 2) * 4 + column
        mail.arrived(res_at(dz, column, k), r_recv.at[sem, k])

    for k in range(4):
        mail.arrived(mix_xr.at[k], m_recv.at[1, k])
        mine = lanes(p.column * cols, cols)
        total = both(k, 0) + mix_xr[k].astype(jnp.float32)
        total = total + tokens[piece(k), mine].astype(jnp.float32)
        res[p.zl, piece(k), mine] = total.astype(jnp.bfloat16)
        res_send(0, p.column, k, 0, p.to_x)
        res_send(0, p.column, k, 1, p.to_zl)
        res_send(0, p.column, k, 2, p.to_c)
        if k > 1:
            g_gu[k - 2].on_zl()

    across = column_of(1, 0)

    def on_x(k):
        res_wait(0, across, k)
        res_send(0, across, k, 5, p.to_c)

    def on_z(k):
        res_wait(1, p.column, k)
        res_send(1, p.column, k, 3, p.to_x)
        res_send(1, p.column, k, 4, p.to_c)

    def on_both(k):
        res_wait(1, across, k)
        res_send(1, across, k, 6, p.to_c)

    on_x(0)
    g_gu[0].on_zh(0)
    on_x(1)
    g_gu[1].on_zh(0)
    on_x(2)
    on_z(0)
    on_x(3)
    on_z(1)
    g_gu[0].on_zh(1)
    g_dn.start_zl(dn_other)
    g_gu[1].on_zh(1)
    g_dn.start_zh(kept(4)(p.index))
    on_z(2)
    on_both(0)
    on_both(1)
    for k in range(4):
        for dx in (0, 1):
            res_wait(0, column_of(dx, 1), k)
    g_gu[0].rows_y()

    def hidden_rows(dz, *halves):
        def body(i, _):
            at = pl.ds(pl.multiple_of(i * chunk, 16), chunk)
            z = (p.zl + dz) % 2
            wide, scale = normed(res[z, at, :].astype(jnp.float32), gain_ffn)
            for q in halves:
                value = jnp.dot(wide, gu_all[q], preferred_element_type=jnp.float32) * scale
                gate, up = value[:, :half], value[:, half:]
                unit = gate / (1.0 + jnp.exp(-gate)) * up
                hid[z, at, q * half:(q + 1) * half] = unit.astype(jnp.bfloat16)
            return 0

        return body

    lax.fori_loop(0, 4, hidden_rows(0, 0), 0)
    on_z(3)
    for k in (0, 1):
        for dx in (0, 1):
            res_wait(1, column_of(dx, 1), k)
    lax.fori_loop(0, 2, hidden_rows(1, 0), 0)
    g_gu[1].rows_y()
    lax.fori_loop(0, 1, hidden_rows(0, 1), 0)
    g_dn.on_zl()
    on_both(2)
    lax.fori_loop(1, 4, hidden_rows(0, 1), 0)
    g_dn.on_zh(0)
    lax.fori_loop(0, 2, hidden_rows(1, 1), 0)
    on_both(3)

    mail.settle(passed)

    def mine(group):
        return (p.c + p.zl + group) % 2 == 0

    def unit(dy, dz, k):
        return dy * 4 + dz * 2 + k

    def sum_own(u, dx):
        return tokens.at[pl.ds((u % 2) * tall, tall), pl.ds((u // 2 * 2 + dx) * block, block)]

    def pair(u, dx):
        return sum_own(u, dx)[...].astype(jnp.float32) + sum_cr[u, dx].astype(jnp.float32)

    def out_part(dy, k):
        return pl.ds(k * tall, tall), lanes((p.y + dy) % 2 * block, block)

    c_copies = [
        mail.make(sum_cs.at[u], sum_cr.at[u], c_send.at[u], c_recv.at[u], p.to_c) for u in range(8)
    ]

    def flow(dy, k, d):
        return dy * 4 + k * 2 + d

    def z_out(n):
        return mask.at[pl.ds((n % 2) * tall, tall), pl.ds((n // 2) * block, block)]

    x_copies = [
        mail.make(sum_xs.at[n], sum_xr.at[n], x_send.at[n], x_recv.at[n], p.to_x) for n in range(8)
    ]
    z_copies = [
        mail.make(z_out(n), sum_zr.at[n], z_send.at[n], z_recv.at[n], p.to_zl) for n in range(8)
    ]
    mail.started += c_copies
    for n in range(8):
        over_x = (n // 4, n // 2 % 2) in X_FIRST
        mail.started += x_copies[n:n + 1] if over_x or n % 2 == 0 else []
        mail.started += z_copies[n:n + 1] if not over_x or n % 2 == 0 else []
    results = [
        pltpu.make_async_copy(
            done.at[out_part(n // 2, n % 2)], out.at[out_part(n // 2, n % 2)], local_sem.at[n]
        )
        for n in range(4)
    ]

    def stage_core(group, dy, dz, k):
        u = unit(dy, dz, k)

        def term(dx):
            j = (((p.x + dx) % 2) * 2 + (p.zl + group) % 2) * 2 + (p.y + dy) % 2
            part = hid[(p.zl + dz) % 2, pl.ds(k * tall, tall), :]
            value = jnp.dot(part, dn_all[j], preferred_element_type=jnp.float32)
            return value.astype(jnp.bfloat16)

        @pl.when(mine(group))
        def _():
            for dx in (0, 1):
                sum_own(u, dx)[...] = term(dx)

        @pl.when(mine(1 - group))
        def _():
            for dx in (0, 1):
                sum_cs[u, dx] = term(dx)
            c_copies[u].start()

    def stage_first(group, dy, dz, k):
        u = unit(dy, dz, k)
        over_x = (dy, k) in X_FIRST

        @pl.when(mine(group))
        def _():
            mail.arrived(sum_cr.at[u], c_recv.at[u])
            if over_x:
                n = flow(dy, k, dz)
                sum_xs[n] = pair(u, 1).astype(jnp.bfloat16)
                x_copies[n].start()
            elif dz == 1:
                for dx in (1, 0):
                    n = flow(dy, k, dx)
                    z_out(n)[...] = pair(u, dx).astype(jnp.bfloat16)
                    z_copies[n].start()

    def stage_second(group, dy, k):
        direct, onward = flow(dy, k, 1), flow(dy, k, 0)
        over_x = (dy, k) in X_FIRST

        @pl.when(mine(group))
        def _():
            if over_x:
                mail.arrived(sum_xr.at[direct], x_recv.at[direct])
                total = pair(unit(dy, 1, k), 0) + sum_xr[direct].astype(jnp.float32)
                z_out(onward)[...] = total.astype(jnp.bfloat16)
                z_copies[onward].start()
            else:
                mail.arrived(sum_zr.at[direct], z_recv.at[direct])
                total = pair(unit(dy, 0, k), 1) + sum_zr[direct].astype(jnp.float32)
                sum_xs[onward] = total.astype(jnp.bfloat16)
                x_copies[onward].start()

    def stage_last(dy, k):
        n = flow(dy, k, 0)
        mail.arrived(sum_xr.at[n], x_recv.at[n])
        mail.arrived(sum_zr.at[n], z_recv.at[n])
        total = pair(unit(dy, 0, k), 0)
        total = total + sum_xr[n].astype(jnp.float32) + sum_zr[n].astype(jnp.float32)
        at = pl.ds(k * tall, tall)
        side = p.column * cols + (p.y + dy) % 2 * block
        total = total + res[p.zl, at, lanes(side, block)].astype(jnp.float32)
        done[out_part(dy, k)] = total.astype(jnp.bfloat16)
        results[dy * 2 + k].start()

    order = [(1, 0), (0, 0), (1, 1), (0, 1)]

    def stage_all(group, dy):
        for n, (dz, k) in enumerate(order):
            stage_core(group, dy, dz, k)
            if n > 1:
                stage_first(group, dy, *order[n - 2])
        for n in (2, 3):
            stage_first(group, dy, *order[n])

    stage_core(0, 0, 0, 0)
    stage_core(0, 0, 0, 1)
    for k in (2, 3):
        for dx in (0, 1):
            res_wait(1, column_of(dx, 1), k)
    lax.fori_loop(2, 3, hidden_rows(1, 0, 1), 0)
    stage_first(0, 0, 0, 0)
    stage_first(0, 0, 0, 1)
    lax.fori_loop(3, 4, hidden_rows(1, 0, 1), 0)
    stage_core(0, 0, 1, 0)
    stage_core(0, 0, 1, 1)
    stage_first(0, 0, 1, 0)
    stage_first(0, 0, 1, 1)
    g_dn.on_zh(1)
    g_dn.rows_y((0,))
    stage_all(0, 1)
    stage_all(1, 0)
    for k in (0, 1):
        if (0, k) in X_FIRST:
            stage_second(0, 0, k)
    g_dn.rows_y((1,))
    stage_all(1, 1)
    for dy, k in ((0, 0), (0, 1), (1, 0), (1, 1)):
        if dy or (0, k) not in X_FIRST:
            stage_second(0, dy, k)
    for dy, k in ((0, 0), (0, 1), (1, 0), (1, 1)):
        stage_second(1, dy, k)
    for dy in (0, 1):
        for k in (0, 1):
            stage_last(dy, k)
    mail.close()
    for copy in results:
        copy.wait()


def paired(mesh):
    fs, tp = mesh.shape["fs"], mesh.shape["tp"]

    def local(
        tokens,
        mix_gain,
        in_weight,
        in_scale,
        out_weight,
        out_scale,
        ffn_gain,
        gate_weight,
        gate_scale,
        up_weight,
        up_scale,
        down_weight,
        down_scale,
    ):
        rows, cols = tokens.shape
        depth, block = in_weight.shape
        wide = gate_weight.shape[1]
        features = cols * tp
        low_type = jnp.bfloat16
        tall = rows // 2
        buffers = [
            ((rows, features), low_type),
            ((2, rows, features), low_type),
            ((features, block), low_type),
            ((fs, block, block), low_type),
            ((2, features, wide // 2), low_type),
            ((fs, wide // 2, block), low_type),
            ((2, rows, wide // 2), low_type),
            ((rows, rows), low_type),
            ((rows, block), jnp.float32),
            ((rows, block), low_type),
            ((rows, block), low_type),
            ((rows, block), low_type),
            ((4, 2, rows // 4, cols), low_type),
            ((4, 2, rows // 4, cols), low_type),
            ((4, 2, rows // 4, cols), low_type),
            ((4, rows // 4, cols), low_type),
            ((4, rows // 4, cols), low_type),
            ((8, 2, tall, block), low_type),
            ((8, 2, tall, block), low_type),
            ((8, tall, block), low_type),
            ((8, tall, block), low_type),
            ((8, tall, block), low_type),
            ((rows, cols), low_type),
            (in_weight.shape, jnp.float32),
            (out_weight.shape, jnp.float32),
            (gate_weight.shape, jnp.float32),
            (up_weight.shape, jnp.float32),
            (down_weight.shape, jnp.float32),
            ((2, depth, wide // 2), low_type),
            ((wide // 2, block), low_type),
        ]
        semaphores = [(6,), (5, 7), (5, fs), (3, 4), (tp, 4), (7, 4), (2 * tp, 4), (2, 4), (2, 4)]
        semaphores += [(8,)] * 6
        anywhere = pl.BlockSpec(memory_space=pl.ANY)
        inside = pl.BlockSpec(memory_space=pltpu.VMEM)
        vectors = (mix_gain, ffn_gain, in_scale, out_scale, gate_scale, up_scale, down_scale)
        return pl.pallas_call(
            fused,
            out_shape=jax.ShapeDtypeStruct((rows, cols), low_type),
            in_specs=[anywhere] * 6 + [inside] * len(vectors),
            out_specs=anywhere,
            scratch_shapes=[pltpu.VMEM(shape, kind) for shape, kind in buffers]
            + [pltpu.SemaphoreType.DMA(shape) for shape in semaphores],
            compiler_params=pltpu.CompilerParams(
                collective_id=0, has_side_effects=True, vmem_limit_bytes=67043328
            ),
        )(
            tokens,
            in_weight,
            out_weight,
            gate_weight,
            up_weight,
            down_weight,
            *vectors,
        )

    return jax.shard_map(
        local, mesh=mesh, in_specs=IN_SPECS, out_specs=P("fs", "tp"), check_vma=False
    )


def solution(mesh):
    fs, tp = mesh.shape["fs"], mesh.shape["tp"]
    xs = max(tp // 2, 1)
    return paired(mesh) if (xs, fs // xs) == (2, 4) else general(mesh)
```
